256 devices in a mesh: sp: 64 (over z, x, core), tp: 4 (over y).
Axes of the slice: x: 4, y: 4, z: 8, core: 2. Of those that a mesh axis runs over, the one named last changes fastest.
Arguments:
- cotangent: bfloat16 [16384, 2048], P('sp'), may hold values from -16 to 16
- route_ids: int32 [16384, 2], P('sp'), may hold values from 0 to 63, all different within a row; in each aligned block of 256 rows (0 to 255, 256 to 511, ...) at most 16 rows name the same one
- route_weights: float32 [16384, 2], P('sp'), may hold values from 0.2 to 1
- expert_inputs: bfloat16 [64, 1024, 2048], P('sp'), may hold values from -6 to 6
- gate_weight: bfloat16 [64, 2048, 1024], P('sp', None, 'tp'), may hold values from -0.125 to 0.125
- up_weight: bfloat16 [64, 2048, 1024], P('sp', None, 'tp'), may hold values from -0.125 to 0.125
- down_weight: bfloat16 [64, 1024, 2048], P('sp', 'tp'), may hold values from -0.1875 to 0.1875
- out_weight: bfloat16 [2048, 512], P(None, 'tp'), may hold values from -0.25 to 0.25
- gate_in: bfloat16 [16384, 512], P('sp', 'tp'), may hold values from -6 to 6
- conv_sum: bfloat16 [16384, 512], P('sp', 'tp'), may hold values from -6 to 6
- conv_c: bfloat16 [16384, 512], P('sp', 'tp'), may hold values from -6 to 6
- conv_v: bfloat16 [16384, 512], P('sp', 'tp'), may hold values from -6 to 6
- conv_taps: float32 [3, 512], P(None, 'tp'), may hold values from -3 to 3
Outputs:
- grad_input: bfloat16 [16384, 2048], P('sp', 'tp')
- grad_gate: bfloat16 [64, 2048, 1024], P('sp', None, 'tp')
- grad_up: bfloat16 [64, 2048, 1024], P('sp', None, 'tp')
- grad_down: bfloat16 [64, 1024, 2048], P('sp', 'tp')
- grad_out_weight: float32 [2048, 512], P('sp', 'tp')
- grad_gate_in: bfloat16 [16384, 512], P('sp', 'tp')
- grad_conv_c: bfloat16 [16384, 512], P('sp', 'tp')
- grad_conv_v: bfloat16 [16384, 512], P('sp', 'tp')
The draws below stay inside these ranges and needn't reach their ends.
Inputs may be any that keep to these rules, and one draw needn't show every extreme that they name: `route_ids`: the 2 experts of a token differ. Among the 256 tokens of one index of sp no expert is named more than 16 times, and in every draw some expert is named exactly 16 times by the tokens of some index of sp.
All inputs are finite; a program needn't handle non-finite values.
Results may differ from the reference program's by a relative error of at most 0.012.
Values may be sent and summed in bfloat16 or wider, within the bound.
A program may use at most 128 MiB of HBM per device.

```python
import math
import jax
import jax.numpy as jnp
import numpy as np
from jax import lax

D = 2048
F = 1024
W = 512
TOP = 2
TAPS = 3
TOK_DEV = 256
EXPERTS = 64
CAP = 16
TOKENS = 16384
N_SP = 64
N_TP = 4


def spiked(result, rng, source, target, parts, factor):
    owner, partner = [(jnp.arange(result.shape[dim]) // (result.shape[dim] // parts)).reshape([-1 if axis == dim else 1 for axis in range(result.ndim)]) for dim in (source, target)]
    chosen = jax.random.permutation(rng, parts)[partner]
    strong = (owner == chosen) | (owner == (partner + parts // 2) % parts)
    return jnp.where(strong, factor * result, result)


def shard_levels(stream_key, extent, cuts, smallest, largest):
    def one(position, blocks):
        heights = jax.random.uniform(jax.random.fold_in(jax.random.fold_in(stream_key, 6), position), (blocks,), jnp.float32, smallest / len(cuts), largest / len(cuts))
        return jnp.repeat(jnp.exp(heights), extent[position] // blocks).reshape((-1,) + (1,) * (len(extent) - position - 1))

    gain = one(*cuts[0])
    for cut in cuts[1:]:
        gain = gain * one(*cut)
    return gain


def deal_out(own_key, own, number, rows, number_of, top, most, lean):
    order = jax.random.permutation(own_key, number_of)
    packed, ordinary = shares(number_of, rows * top, most, lean, True), shares(number_of, rows * top, most, lean, False)
    places = jnp.arange(number_of)

    def named(sizes, offset_by):
        used = int((sizes > 0).sum())
        fixed = max(1, used // 4)
        passed = fixed + (places - fixed + offset_by * (used - fixed)) % max(1, number_of - fixed)
        return jnp.zeros((number_of,), jnp.int32).at[order[jnp.where(places < fixed, places, passed)]].set(jnp.asarray(sizes, jnp.int32))

    sizes = jnp.where(number % 4 == 0, named(packed, number // 4), named(ordinary, number - number // 4 - 1))
    mixed = jax.random.permutation(jax.random.fold_in(own, 3), number_of)
    giver, receiver = mixed[0:number_of // 2 * 2:2], mixed[1:number_of // 2 * 2:2]
    room = jnp.minimum(sizes[giver] - 1, most - sizes[receiver]) // 2
    room = jnp.where((giver == order[0]) | (receiver == order[0]) | (sizes[receiver] == 0), 0, jnp.maximum(room, 0))
    passed = jax.random.randint(jax.random.fold_in(own, 4), (number_of // 2,), 0, 1 << 20) % (room + 1)
    sizes = sizes.at[giver].add(-passed).at[receiver].add(passed)
    labels = jnp.searchsorted(jnp.cumsum(sizes), jnp.arange(rows * top), side="right").astype(jnp.int32)
    table = labels.reshape(top, rows).T
    table = table[jax.random.permutation(jax.random.fold_in(own, 1), rows)]
    offset_by = jax.random.randint(jax.random.fold_in(own, 2), (rows, 1), 0, top)
    return jnp.take_along_axis(table, (jnp.arange(top)[None, :] + offset_by) % top, axis=1)


def shares(amount, total, bound, slope, full):
    loads = [(1 << 20) // math.isqrt(grade ** slope) + 1 for grade in range(1, amount + 1)]
    largest = bound if full else min(bound, max(-(-total // amount), total * loads[0] // sum(loads)))
    least = 1 if total - largest >= amount - 1 else 0
    counts, spare = [largest] + [least] * (amount - 1), total - largest - least * (amount - 1)
    while spare > 0:
        free = [i for i in range(1, amount) if counts[i] < largest] or [i for i in range(1, amount) if counts[i] < bound]
        mass, remaining = sum([loads[i] for i in free]), spare
        for i in free:
            more = min(bound - counts[i], max(1, remaining * loads[i] // mass), spare)
            counts[i] = counts[i] + more
            spare = spare - more
    return np.array(counts)


def scatter_about(stream_key, extent, scale, bound, split=(), kind=jnp.bfloat16):
    result = jax.random.normal(stream_key, extent, jnp.float32) * scale
    if len(split) > 0:
        result = shard_levels(stream_key, extent, split, -0.22, 0.18) * result
    return jnp.clip(result, min=-bound, max=bound).astype(kind)


def gaussian_with(own_key, extent, scale, limit, shards, heavy, held_as=jnp.bfloat16):
    array = scale * jax.random.normal(own_key, extent, jnp.float32)
    if shards:
        array = array * shard_levels(own_key, extent, shards, -0.22, 0.18)
    return jnp.clip(spiked(array, jax.random.fold_in(own_key, 3), *heavy), -limit, limit).astype(held_as)


def setup_inputs(seed: int = 0) -> dict:
    key_list = jax.random.split(jax.random.key(seed), 14)
    cotangent = gaussian_with(key_list[0], (TOKENS, D), 1.0, 16.0, ((0, 64),), (0, 1, 64, 4.0))
    route_ids_keys = jax.random.split(jax.random.fold_in(key_list[1], 1), TOKENS // TOK_DEV)
    route_ids_turns = jax.random.permutation(jax.random.fold_in(key_list[1], 3), TOKENS // TOK_DEV)
    route_ids = jax.vmap(lambda own, number: deal_out(jax.random.fold_in(key_list[1], 2), own, number, TOK_DEV, EXPERTS, TOP, CAP, 1))(route_ids_keys, route_ids_turns).reshape((TOKENS, TOP))
    route_weights = jnp.clip(0.2 + 0.8 * jax.random.uniform(key_list[2], (TOKENS, TOP), jnp.float32) ** shard_levels(key_list[2], (TOKENS, TOP), ((0, 64),), -0.2, 0.2), 0.2, 1.0)
    expert_inputs = scatter_about(key_list[3], (EXPERTS, N_SP * CAP, D), 1.0, 6.0, ((0, 64),))
    gate_weight = scatter_about(key_list[4], (EXPERTS, D, F), D ** -0.5, 0.125, ((0, 64), (2, 4)))
    up_weight = scatter_about(key_list[5], (EXPERTS, D, F), D ** -0.5, 0.125, ((0, 64), (2, 4)))
    down_weight = scatter_about(key_list[6], (EXPERTS, F, D), F ** -0.5, 0.1875, ((0, 64), (1, 4)))
    out_weight = scatter_about(key_list[7], (D, W), W ** -0.5, 0.25, ((1, 4),))
    gate_in = scatter_about(key_list[8], (TOKENS, W), 1.0, 6.0, ((0, 64), (1, 4)))
    conv_sum = scatter_about(key_list[9], (TOKENS, W), 1.0, 6.0, ((0, 64), (1, 4)))
    conv_c = scatter_about(key_list[10], (TOKENS, W), 1.0, 6.0, ((0, 64), (1, 4)))
    conv_v = scatter_about(key_list[11], (TOKENS, W), 1.0, 6.0, ((0, 64), (1, 4)))
    conv_taps = scatter_about(key_list[12], (TAPS, W), 0.6, 3.0, ((1, 4),), jnp.float32)
    return dict(cotangent=cotangent, route_ids=route_ids, route_weights=route_weights, expert_inputs=expert_inputs, gate_weight=gate_weight, up_weight=up_weight, down_weight=down_weight, out_weight=out_weight, gate_in=gate_in, conv_sum=conv_sum, conv_c=conv_c, conv_v=conv_v, conv_taps=conv_taps)


def reference(cotangent, route_ids, route_weights, expert_inputs, gate_weight, up_weight, down_weight, out_weight, gate_in, conv_sum, conv_c, conv_v, conv_taps):
    experts = gate_weight.shape[0]
    pair_ids = route_ids.reshape(N_SP, TOK_DEV * TOP)
    onehot = (pair_ids[:, :, None] == jnp.arange(experts, dtype=jnp.int32)[None, None, :]).astype(jnp.int32)
    before = jnp.cumsum(onehot, axis=1) - onehot
    ranked = jnp.sum(before * onehot, axis=2)
    source = jnp.arange(N_SP, dtype=jnp.int32)[:, None]
    slot_row = (source * CAP + ranked).reshape(-1).astype(jnp.int32)
    target = pair_ids.reshape(-1).astype(jnp.int32)
    weighted = (route_weights[:, :, None] * cotangent.astype(jnp.float32)[:, None, :]).astype(jnp.bfloat16).reshape(-1, D)
    routed = jnp.zeros((experts, N_SP * CAP, D), jnp.bfloat16).at[target, slot_row].set(weighted)
    quarter = F // N_TP

    def expert_step(expert_items):
        stored, grad_rows, w_gate, w_up, w_down = expert_items
        pre_gate = jnp.dot(stored, w_gate, preferred_element_type=jnp.float32)
        pre_up = jnp.dot(stored, w_up, preferred_element_type=jnp.float32)
        gate_sig = jax.nn.sigmoid(pre_gate)
        swish_gate = pre_gate * gate_sig
        hidden = (swish_gate * pre_up).astype(jnp.bfloat16)
        grad_hidden = jnp.dot(grad_rows, w_down.T, preferred_element_type=jnp.float32)
        grad_pregate = (grad_hidden * pre_up * gate_sig * (1.0 + pre_gate * (1.0 - gate_sig))).astype(jnp.bfloat16)
        grad_preup = (grad_hidden * swish_gate).astype(jnp.bfloat16)
        grad_down = jnp.dot(hidden.T, grad_rows, preferred_element_type=jnp.float32).astype(jnp.bfloat16)
        grad_gate = jnp.dot(stored.T, grad_pregate, preferred_element_type=jnp.float32).astype(jnp.bfloat16)
        grad_up = jnp.dot(stored.T, grad_preup, preferred_element_type=jnp.float32).astype(jnp.bfloat16)
        total = jnp.zeros((stored.shape[0], D), jnp.float32)
        for part_index in range(N_TP):
            low = part_index * quarter
            high = low + quarter
            part = jnp.dot(grad_pregate[:, low:high], w_gate[:, low:high].T, preferred_element_type=jnp.float32)
            part = part + jnp.dot(grad_preup[:, low:high], w_up[:, low:high].T, preferred_element_type=jnp.float32)
            total = total + lax.optimization_barrier(part.astype(jnp.bfloat16)).astype(jnp.float32)
        return grad_gate, grad_up, grad_down, total.astype(jnp.bfloat16)

    grad_gate, grad_up, grad_down, grad_x = lax.map(expert_step, (expert_inputs, routed, gate_weight, up_weight, down_weight))
    returned = grad_x[target, slot_row].astype(jnp.float32).reshape(TOKENS, TOP, D)
    grad_input = (cotangent.astype(jnp.float32) + jnp.sum(returned, axis=1)).astype(jnp.bfloat16)
    mixed_rows = (gate_in.astype(jnp.float32) * conv_sum.astype(jnp.float32)).astype(jnp.bfloat16)
    grad_mixed = jnp.dot(grad_input, out_weight, preferred_element_type=jnp.float32)
    grad_out_weight = jnp.dot(grad_input.T, mixed_rows, preferred_element_type=jnp.float32)
    grad_gate_in = (grad_mixed * conv_sum.astype(jnp.float32)).astype(jnp.bfloat16)
    grad_sum = grad_mixed * gate_in.astype(jnp.float32)
    extended = jnp.concatenate([grad_sum, jnp.zeros((2, grad_sum.shape[1]), jnp.float32)], axis=0)
    grad_prod = conv_taps[0] * extended[2:] + conv_taps[1] * extended[1:-1] + conv_taps[2] * extended[:-2]
    grad_conv_c = (grad_prod * conv_v.astype(jnp.float32)).astype(jnp.bfloat16)
    grad_conv_v = (grad_prod * conv_c.astype(jnp.float32)).astype(jnp.bfloat16)
    return (grad_input, grad_gate, grad_up, grad_down, grad_out_weight, grad_gate_in, grad_conv_c, grad_conv_v)
```

```python
import functools

import jax
import jax.numpy as jnp
from jax import lax
from jax.experimental import pallas as pl
from jax.experimental.pallas import tpu as pltpu
from jax.sharding import PartitionSpec as P

TOP = 2
MESH = pl.DeviceIdType.MESH
F32 = jnp.float32
BF16 = jnp.bfloat16


def expert_kernel(
    dims,
    out_ref,
    x_hbm,
    gate_hbm,
    up_hbm,
    down_hbm,
    returned,
    g_gate,
    g_up,
    g_down,
    x_v,
    gate_v,
    up_v,
    down_v,
    routed,
    part,
    rs1a,
    rs1b,
    rs2a,
    rs2b,
    ret_src,
    swish_s,
    slope_s,
    hidden_s,
    gpg_s,
    gpu_s,
    load_sem,
    send_z,
    recv_z,
    send_y,
    recv_y,
    send_r,
    recv_r,
):
    sps, tps, chunks, cap = dims
    group = sps // chunks
    rows_c = group * cap
    half = rows_c // 2
    cols = out_ref.shape[1]
    me = lax.axis_index("sp")
    q = lax.axis_index("tp")
    z = me // group
    g = me % group
    up_q = (q + 1) % tps
    dn_q = (q + tps - 1) % tps
    far_q = (q + 2) % tps

    loads = [
        pltpu.make_async_copy(src, dst, load_sem.at[n])
        for n, (src, dst) in enumerate(
            ((x_hbm, x_v), (gate_hbm, gate_v), (up_hbm, up_v), (down_hbm, down_v))
        )
    ]
    for load in loads:
        load.start()

    barrier = pltpu.get_barrier_semaphore()

    def greet(k, carry):
        pl.semaphore_signal(
            barrier, inc=1, device_id=((me + k) % sps, q), device_id_type=MESH
        )
        return carry

    lax.fori_loop(1, sps, greet, 0)
    for peer in (up_q, dn_q):
        pl.semaphore_signal(barrier, inc=1, device_id=(me, peer), device_id_type=MESH)
    pl.semaphore_wait(barrier, sps - 1 + 2)

    def offset(i):
        return ((i + 1) // 2) * (2 * (i % 2) - 1)

    def chunk_start(i):
        return ((z - offset(i) + chunks) % chunks) * rows_c

    def block_copy(i, k):
        peer = ((z + offset(i) + chunks) % chunks) * group + (g + k) % group
        return pltpu.make_async_remote_copy(
            src_ref=out_ref.at[pl.ds(pl.multiple_of(peer * cap, cap), cap), :],
            dst_ref=routed.at[q, pl.ds(pl.multiple_of(me * cap, cap), cap), :],
            send_sem=send_z.at[i],
            recv_sem=recv_z.at[i],
            device_id=(peer, q),
            device_id_type=MESH,
        )

    def send_first(k, carry):
        block_copy(0, k).start()
        return carry

    lax.fori_loop(1, group, send_first, 0)

    def send_chunk(i, carry):
        def send_one(k, inner):
            block_copy(i, k).start()
            return inner

        return lax.fori_loop(0, group, send_one, carry)

    lax.fori_loop(1, chunks, send_chunk, 0)
    own = pl.ds(pl.multiple_of(me * cap, cap), cap)
    routed[q, own, :] = out_ref[own, :]

    for load in loads:
        load.wait()
    pre_rows = 2 * rows_c

    def forward(b, carry):
        rows = pl.ds(pl.multiple_of(b * pre_rows, pre_rows), pre_rows)
        pre_gate = jnp.dot(x_v[rows, :], gate_v[...], preferred_element_type=F32)
        pre_up = jnp.dot(x_v[rows, :], up_v[...], preferred_element_type=F32)
        sig = jax.nn.sigmoid(pre_gate)
        swish = pre_gate * sig
        swish_s[rows, :] = swish
        slope_s[rows, :] = pre_up * sig * (1.0 + pre_gate * (1.0 - sig))
        hidden_s[rows, :] = (swish * pre_up).astype(BF16)
        return carry

    lax.fori_loop(0, sps * cap // pre_rows, forward, 0)

    def at(i, first=0, size=None):
        return pl.ds(pl.multiple_of(chunk_start(i) + first, half), size or rows_c)

    def y_copy(src, dst, kind, i, peer):
        return pltpu.make_async_remote_copy(
            src_ref=src,
            dst_ref=dst,
            send_sem=send_y.at[kind, i],
            recv_sem=recv_y.at[kind, i],
            device_id=(me, peer),
            device_id_type=MESH,
        )

    def gather_up(i):
        ref = routed.at[q, at(i), :]
        return y_copy(ref, ref, 0, i, up_q)

    def gather_dn(i):
        ref = routed.at[q, at(i), :]
        return y_copy(ref, ref, 1, i, dn_q)

    def pass_up(i):
        ref = routed.at[dn_q, at(i, 0, half), :]
        return y_copy(ref, ref, 2, i, up_q)

    def pass_dn(i):
        ref = routed.at[up_q, at(i, half, half), :]
        return y_copy(ref, ref, 3, i, dn_q)

    def first_up(i):
        return y_copy(part.at[far_q, at(i, 0, half), :], rs1a.at[i], 4, i, up_q)

    def first_dn(i):
        return y_copy(part.at[far_q, at(i, half, half), :], rs1b.at[i], 5, i, dn_q)

    def last_up(i):
        return y_copy(part.at[up_q, at(i), :], rs2a.at[i], 6, i, up_q)

    def last_dn(i):
        return y_copy(part.at[dn_q, at(i), :], rs2b.at[i], 7, i, dn_q)

    every = (gather_up, gather_dn, pass_up, pass_dn, first_up, first_dn, last_up, last_dn)

    def wait_z(i, count):
        rows = pl.ds(0, count * cap)
        pltpu.make_async_remote_copy(
            src_ref=out_ref.at[rows, :],
            dst_ref=routed.at[q, rows, :],
            send_sem=send_z.at[i],
            recv_sem=recv_z.at[i],
            device_id=(me, up_q),
            device_id_type=MESH,
        ).wait_recv()

    def stage_gather(i):
        @pl.when(i == 0)
        def _():
            wait_z(i, group - 1)

        @pl.when(i > 0)
        def _():
            wait_z(i, group)

        gather_up(i).start()
        gather_dn(i).start()

    def stage_pass(i):
        gather_up(i).wait_recv()
        pass_up(i).start()
        gather_dn(i).wait_recv()
        pass_dn(i).start()

    def stage_compute(i):
        pass_up(i).wait_recv()
        pass_dn(i).wait_recv()
        rows = at(i)
        grad_hidden = jnp.zeros((rows_c, down_v.shape[0]), F32)
        for lane in range(tps):
            grad_hidden += lax.dot_general(
                routed[lane, rows, :],
                down_v[:, lane * cols : (lane + 1) * cols],
                (((1,), (1,)), ((), ())),
                preferred_element_type=F32,
            )
        gpg = (grad_hidden * slope_s[rows, :]).astype(BF16)
        gpu = (grad_hidden * swish_s[rows, :]).astype(BF16)
        gpg_s[rows, :] = gpg
        gpu_s[rows, :] = gpu
        for lane in range(tps):
            span = slice(lane * cols, (lane + 1) * cols)
            piece = lax.dot_general(
                gpg, gate_v[span, :], (((1,), (1,)), ((), ())), preferred_element_type=F32
            )
            piece += lax.dot_general(
                gpu, up_v[span, :], (((1,), (1,)), ((), ())), preferred_element_type=F32
            )
            part[lane, rows, :] = piece.astype(BF16)
        first_up(i).start()
        first_dn(i).start()

    def stage_first(i):
        lower, upper = at(i, 0, half), at(i, half, half)
        first_up(i).wait_recv()
        part[up_q, lower, :] = (
            part[up_q, lower, :].astype(F32) + rs1a[i].astype(F32)
        ).astype(BF16)
        last_up(i).start()
        first_dn(i).wait_recv()
        part[dn_q, upper, :] = (
            part[dn_q, upper, :].astype(F32) + rs1b[i].astype(F32)
        ).astype(BF16)
        last_dn(i).start()

    def return_copy(i, k):
        source = ((z - offset(i) + chunks) % chunks) * group + (g + k) % group
        return pltpu.make_async_remote_copy(
            src_ref=ret_src.at[pl.ds(pl.multiple_of(source * cap, cap), cap), :],
            dst_ref=returned.at[own, :],
            send_sem=send_r,
            recv_sem=recv_r,
            device_id=(source, q),
            device_id_type=MESH,
        )

    def stage_return(i):
        rows = at(i)
        last_up(i).wait_recv()
        last_dn(i).wait_recv()
        total = part[q, rows, :].astype(F32) + rs2a[i].astype(F32) + rs2b[i].astype(F32)
        ret_src[rows, :] = total.astype(BF16)

        @pl.when(i > 0)
        def _():
            return_copy(i, 0).start()

        def send_one(k, carry):
            return_copy(i, k).start()
            return carry

        lax.fori_loop(1, group, send_one, 0)

    stages = (stage_gather, stage_pass, stage_compute, stage_first, stage_return)

    def step(t, carry):
        for depth, stage in reversed(tuple(enumerate(stages))):
            i = t - depth

            @pl.when((i >= 0) & (i < chunks))
            def _():
                stage(i)

        return carry

    lax.fori_loop(0, chunks + len(stages) - 1, step, 0)
    returned[own, :] = ret_src[own, :]

    contract0 = (((0,), (0,)), ((), ()))
    for lane in range(tps):
        span = slice(lane * cols, (lane + 1) * cols)
        g_down[:, span] = lax.dot_general(
            hidden_s[...], routed[lane], contract0, preferred_element_type=F32
        ).astype(BF16)
        g_gate[span, :] = lax.dot_general(
            x_v[:, span], gpg_s[...], contract0, preferred_element_type=F32
        ).astype(BF16)
        g_up[span, :] = lax.dot_general(
            x_v[:, span], gpu_s[...], contract0, preferred_element_type=F32
        ).astype(BF16)

    def drain(i, carry):
        for copy in every:
            copy(i).wait_send()
        return carry

    lax.fori_loop(0, chunks, drain, 0)

    def drain_z(i, count):
        rows = pl.ds(0, count * cap)
        pltpu.make_async_remote_copy(
            src_ref=out_ref.at[rows, :],
            dst_ref=routed.at[q, rows, :],
            send_sem=send_z.at[i],
            recv_sem=recv_z.at[i],
            device_id=(me, up_q),
            device_id_type=MESH,
        ).wait_send()

    drain_z(0, group - 1)

    def drain_rest(i, carry):
        drain_z(i, group)
        return carry

    lax.fori_loop(1, chunks, drain_rest, 0)
    rest = pl.ds(0, (sps - 1) * cap)
    final = pltpu.make_async_remote_copy(
        src_ref=ret_src.at[rest, :],
        dst_ref=returned.at[rest, :],
        send_sem=send_r,
        recv_sem=recv_r,
        device_id=(me, up_q),
        device_id_type=MESH,
    )
    final.wait_send()
    final.wait_recv()


def run_experts(dims, outgoing, x, gate, up, down):
    sps, tps, chunks, cap = dims
    rows, cols = outgoing.shape
    width, units = gate.shape
    rows_c = rows // chunks
    vmem = pl.BlockSpec(memory_space=pltpu.VMEM)
    hbm = pl.BlockSpec(memory_space=pltpu.HBM)
    scratch = [
        pltpu.VMEM((rows, width), BF16),
        pltpu.VMEM((width, units), BF16),
        pltpu.VMEM((width, units), BF16),
        pltpu.VMEM((units, width), BF16),
        pltpu.VMEM((tps, rows, cols), BF16),
        pltpu.VMEM((tps, rows, cols), BF16),
        pltpu.VMEM((chunks, rows_c // 2, cols), BF16),
        pltpu.VMEM((chunks, rows_c // 2, cols), BF16),
        pltpu.VMEM((chunks, rows_c, cols), BF16),
        pltpu.VMEM((chunks, rows_c, cols), BF16),
        pltpu.VMEM((rows, cols), BF16),
        pltpu.VMEM((rows, units), F32),
        pltpu.VMEM((rows, units), F32),
        pltpu.VMEM((rows, units), BF16),
        pltpu.VMEM((rows, units), BF16),
        pltpu.VMEM((rows, units), BF16),
        pltpu.SemaphoreType.DMA((4,)),
        pltpu.SemaphoreType.DMA((chunks,)),
        pltpu.SemaphoreType.DMA((chunks,)),
        pltpu.SemaphoreType.DMA((8, chunks)),
        pltpu.SemaphoreType.DMA((8, chunks)),
        pltpu.SemaphoreType.DMA,
        pltpu.SemaphoreType.DMA,
    ]
    return pl.pallas_call(
        functools.partial(expert_kernel, dims),
        out_shape=(
            jax.ShapeDtypeStruct((rows, cols), BF16),
            jax.ShapeDtypeStruct((width, units), BF16),
            jax.ShapeDtypeStruct((width, units), BF16),
            jax.ShapeDtypeStruct((units, width), BF16),
        ),
        in_specs=[vmem, hbm, hbm, hbm, hbm],
        out_specs=(vmem, vmem, vmem, vmem),
        scratch_shapes=scratch,
        compiler_params=pltpu.CompilerParams(
            collective_id=0, has_side_effects=True, vmem_limit_bytes=60 * 1024 * 1024
        ),
        name="experts",
    )(outgoing, x, gate, up, down)


def split_up(value, dim, peers):
    before, after = (value.shape[:dim], value.shape[dim + 1 :])
    return jnp.moveaxis(value.reshape(*before, peers, -1, *after), dim, 0)


def collect(value, axis, dim):
    copies = jnp.broadcast_to(value, (lax.axis_size(axis), *value.shape))
    pieces = lax.all_to_all(copies, axis, split_axis=0, concat_axis=0, tiled=True)
    shape = list(value.shape)
    shape[dim] *= pieces.shape[0]
    return jnp.moveaxis(pieces, 0, dim).reshape(shape)


def summed_on_arrival(value, axis, dim):
    pieces = split_up(value, dim, lax.axis_size(axis))
    arrived = lax.all_to_all(pieces, axis, split_axis=0, concat_axis=0, tiled=True)
    return arrived.astype(F32).sum(axis=0)


def shifted(block, axis, distance):
    devices = range(lax.axis_size(axis))
    route = [(i - distance, i) for i in devices if i - distance in devices]
    return lax.ppermute(block, axis, route)


def routing(route_ids, route_weights, experts, capacity):
    tokens = route_ids.shape[0]
    ids = route_ids.T
    weights = route_weights.T
    names = lax.broadcasted_iota(jnp.int32, (experts, tokens), 0)
    first, second = names == ids[0][None, :], names == ids[1][None, :]
    weight = jnp.where(first, weights[0][None, :], 0.0) + jnp.where(
        second, weights[1][None, :], 0.0
    )
    named = first | second
    earlier = lax.broadcasted_iota(jnp.int32, (tokens, tokens), 0) < lax.broadcasted_iota(
        jnp.int32, (tokens, tokens), 1
    )
    rank = jnp.dot(named.astype(BF16), earlier.astype(BF16), preferred_element_type=F32)
    rank = jnp.where(named, rank.astype(jnp.int32), -1)
    slots = lax.broadcasted_iota(jnp.int32, (experts, capacity, tokens), 1)
    chosen = rank[:, None, :] == slots
    slot_weight = jnp.sum(jnp.where(chosen, weight[:, None, :], 0.0), axis=2)
    return chosen.reshape(experts * capacity, tokens).astype(BF16), slot_weight.reshape(-1, 1)


def body(
    chunks,
    cotangent,
    route_ids,
    route_weights,
    expert_inputs,
    gate_weight,
    up_weight,
    down_weight,
    out_weight,
    gate_in,
    conv_sum,
    conv_c,
    conv_v,
    conv_taps,
):
    groups = lax.axis_size("sp")
    lanes = lax.axis_size("tp")
    capacity = expert_inputs.shape[1] // groups
    experts = groups
    model_width = cotangent.shape[1]
    lane_cols = model_width // lanes
    own_rows = lax.dynamic_slice_in_dim(cotangent, lax.axis_index("tp") * lane_cols, lane_cols, 1)
    chosen, slot_weight = routing(route_ids, route_weights, experts, capacity)
    picked = jnp.dot(chosen, own_rows, preferred_element_type=F32)
    outgoing = (slot_weight * picked).astype(BF16)
    returned, grad_gate, grad_up, grad_down = run_experts(
        (groups, lanes, chunks, capacity),
        outgoing,
        expert_inputs[0],
        gate_weight[0],
        up_weight[0],
        down_weight[0],
    )
    returned_sum = lax.dot_general(
        chosen, returned, (((0,), (0,)), ((), ())), preferred_element_type=F32
    )
    grad_input = (own_rows.astype(F32) + returned_sum).astype(BF16)
    full_mid = collect(grad_input, "tp", 1)
    mixed_rows = (gate_in.astype(F32) * conv_sum.astype(F32)).astype(BF16)
    grad_mixed = jnp.dot(full_mid, out_weight, preferred_element_type=F32)
    grad_out_weight = summed_on_arrival(
        lax.dot_general(
            full_mid, mixed_rows, (((0,), (0,)), ((), ())), preferred_element_type=F32
        ),
        "sp",
        0,
    )
    grad_gate_in = (grad_mixed * conv_sum.astype(F32)).astype(BF16)
    grad_sum = grad_mixed * gate_in.astype(F32)
    next_rows = shifted(grad_sum[:2], "sp", -1)
    extended = jnp.concatenate([grad_sum, next_rows], axis=0)
    grad_prod = (
        conv_taps[0] * extended[2:] + conv_taps[1] * extended[1:-1] + conv_taps[2] * extended[:-2]
    )
    grad_conv_c = (grad_prod * conv_v.astype(F32)).astype(BF16)
    grad_conv_v = (grad_prod * conv_c.astype(F32)).astype(BF16)
    return (
        grad_input,
        grad_gate[None],
        grad_up[None],
        grad_down[None],
        grad_out_weight,
        grad_gate_in,
        grad_conv_c,
        grad_conv_v,
    )


def solution(mesh):
    placed = (
        P("sp", None),
        P("sp", None),
        P("sp", None),
        P("sp", None, None),
        P("sp", None, "tp"),
        P("sp", None, "tp"),
        P("sp", "tp", None),
        P(None, "tp"),
        P("sp", "tp"),
        P("sp", "tp"),
        P("sp", "tp"),
        P("sp", "tp"),
        P(None, "tp"),
    )
    chunks = min(8, mesh.shape["sp"] // 2)
    return jax.shard_map(
        functools.partial(body, chunks),
        mesh=mesh,
        in_specs=placed,
        out_specs=(
            P("sp", "tp"),
            P("sp", None, "tp"),
            P("sp", None, "tp"),
            P("sp", "tp", None),
            P("sp", "tp"),
            P("sp", "tp"),
            P("sp", "tp"),
            P("sp", "tp"),
        ),
        check_vma=False,
    )
```

```python
import functools

import jax
import jax.numpy as jnp
from jax import lax
from jax.experimental import pallas as pl
from jax.experimental.pallas import tpu as pltpu
from jax.sharding import PartitionSpec as P

TOP = 2
MESH = pl.DeviceIdType.MESH
F32 = jnp.float32
BF16 = jnp.bfloat16


def step_kernel(
    dims,
    out_ref,
    chosen,
    own_rows,
    out_weight,
    gate_in,
    conv_sum,
    conv_c,
    conv_v,
    taps,
    x_hbm,
    gate_hbm,
    up_hbm,
    down_hbm,
    grad_input,
    g_gate,
    g_up,
    g_down,
    g_out,
    g_gate_in,
    g_conv_c,
    g_conv_v,
    returned,
    chosen_t,
    full_in,
    mixed,
    sums,
    out_terms,
    out_in,
    x_v,
    gate_v,
    up_v,
    down_v,
    routed,
    part,
    rs1a,
    rs1b,
    rs2a,
    rs2b,
    ret_src,
    swish_s,
    slope_s,
    hidden_s,
    gpg_s,
    gpu_s,
    load_sem,
    send_z,
    recv_z,
    send_y,
    recv_y,
    send_r,
    recv_r,
    send_s,
    recv_s,
    send_o,
    recv_o,
    send_n,
    recv_n,
):
    sps, tps, chunks, cap = dims
    group = sps // chunks
    rows_c = group * cap
    half = rows_c // 2
    cols = out_ref.shape[1]
    me = lax.axis_index("sp")
    q = lax.axis_index("tp")
    z = me // group
    g = me % group
    up_q = (q + 1) % tps
    dn_q = (q + tps - 1) % tps
    far_q = (q + 2) % tps

    loads = [
        pltpu.make_async_copy(src, dst, load_sem.at[n])
        for n, (src, dst) in enumerate(
            ((x_hbm, x_v), (gate_hbm, gate_v), (up_hbm, up_v), (down_hbm, down_v))
        )
    ]
    for load in loads:
        load.start()

    barrier = pltpu.get_barrier_semaphore()

    def greet(k, carry):
        pl.semaphore_signal(
            barrier, inc=1, device_id=((me + k) % sps, q), device_id_type=MESH
        )
        return carry

    lax.fori_loop(1, sps, greet, 0)
    for peer in (up_q, dn_q):
        pl.semaphore_signal(barrier, inc=1, device_id=(me, peer), device_id_type=MESH)
    pl.semaphore_wait(barrier, sps - 1 + 2)

    def offset(i):
        return ((i + 1) // 2) * (2 * (i % 2) - 1)

    def chunk_start(i):
        return ((z - offset(i) + chunks) % chunks) * rows_c

    def block_copy(i, k):
        peer = ((z + offset(i) + chunks) % chunks) * group + (g + k) % group
        return pltpu.make_async_remote_copy(
            src_ref=out_ref.at[pl.ds(pl.multiple_of(peer * cap, cap), cap), :],
            dst_ref=routed.at[q, pl.ds(pl.multiple_of(me * cap, cap), cap), :],
            send_sem=send_z.at[i],
            recv_sem=recv_z.at[i],
            device_id=(peer, q),
            device_id_type=MESH,
        )

    def send_first(k, carry):
        block_copy(0, k).start()
        return carry

    lax.fori_loop(1, group, send_first, 0)

    def send_chunk(i, carry):
        def send_one(k, inner):
            block_copy(i, k).start()
            return inner

        return lax.fori_loop(0, group, send_one, carry)

    lax.fori_loop(1, chunks, send_chunk, 0)
    own = pl.ds(pl.multiple_of(me * cap, cap), cap)
    routed[q, own, :] = out_ref[own, :]

    chosen_t[...] = chosen[...].T
    mixed[...] = (gate_in[...].astype(F32) * conv_sum[...].astype(F32)).astype(BF16)

    for load in loads:
        load.wait()
    pre_rows = 2 * rows_c

    def forward(b, carry):
        rows = pl.ds(pl.multiple_of(b * pre_rows, pre_rows), pre_rows)
        pre_gate = jnp.dot(x_v[rows, :], gate_v[...], preferred_element_type=F32)
        pre_up = jnp.dot(x_v[rows, :], up_v[...], preferred_element_type=F32)
        sig = jax.nn.sigmoid(pre_gate)
        swish = pre_gate * sig
        swish_s[rows, :] = swish
        slope_s[rows, :] = pre_up * sig * (1.0 + pre_gate * (1.0 - sig))
        hidden_s[rows, :] = (swish * pre_up).astype(BF16)
        return carry

    lax.fori_loop(0, sps * cap // pre_rows, forward, 0)

    def at(i, first=0, size=None):
        return pl.ds(pl.multiple_of(chunk_start(i) + first, half), size or rows_c)

    def y_copy(src, dst, kind, i, peer):
        return pltpu.make_async_remote_copy(
            src_ref=src,
            dst_ref=dst,
            send_sem=send_y.at[kind, i],
            recv_sem=recv_y.at[kind, i],
            device_id=(me, peer),
            device_id_type=MESH,
        )

    def gather_up(i):
        ref = routed.at[q, at(i), :]
        return y_copy(ref, ref, 0, i, up_q)

    def gather_dn(i):
        ref = routed.at[q, at(i), :]
        return y_copy(ref, ref, 1, i, dn_q)

    def pass_up(i):
        ref = routed.at[dn_q, at(i, 0, half), :]
        return y_copy(ref, ref, 2, i, up_q)

    def pass_dn(i):
        ref = routed.at[up_q, at(i, half, half), :]
        return y_copy(ref, ref, 3, i, dn_q)

    def first_up(i):
        return y_copy(part.at[far_q, at(i, 0, half), :], rs1a.at[i], 4, i, up_q)

    def first_dn(i):
        return y_copy(part.at[far_q, at(i, half, half), :], rs1b.at[i], 5, i, dn_q)

    def last_up(i):
        return y_copy(part.at[up_q, at(i), :], rs2a.at[i], 6, i, up_q)

    def last_dn(i):
        return y_copy(part.at[dn_q, at(i), :], rs2b.at[i], 7, i, dn_q)

    every = (gather_up, gather_dn, pass_up, pass_dn, first_up, first_dn, last_up, last_dn)

    def wait_z(i, count):
        rows = pl.ds(0, count * cap)
        pltpu.make_async_remote_copy(
            src_ref=out_ref.at[rows, :],
            dst_ref=routed.at[q, rows, :],
            send_sem=send_z.at[i],
            recv_sem=recv_z.at[i],
            device_id=(me, up_q),
            device_id_type=MESH,
        ).wait_recv()

    def stage_gather(i):
        @pl.when(i == 0)
        def _():
            wait_z(i, group - 1)

        @pl.when(i > 0)
        def _():
            wait_z(i, group)

        gather_up(i).start()
        gather_dn(i).start()

    def stage_pass(i):
        gather_up(i).wait_recv()
        pass_up(i).start()
        gather_dn(i).wait_recv()
        pass_dn(i).start()

    def stage_compute(i):
        pass_up(i).wait_recv()
        pass_dn(i).wait_recv()
        rows = at(i)
        grad_hidden = jnp.zeros((rows_c, down_v.shape[0]), F32)
        for lane in range(tps):
            grad_hidden += lax.dot_general(
                routed[lane, rows, :],
                down_v[:, lane * cols : (lane + 1) * cols],
                (((1,), (1,)), ((), ())),
                preferred_element_type=F32,
            )
        gpg = (grad_hidden * slope_s[rows, :]).astype(BF16)
        gpu = (grad_hidden * swish_s[rows, :]).astype(BF16)
        gpg_s[rows, :] = gpg
        gpu_s[rows, :] = gpu
        for lane in range(tps):
            span = slice(lane * cols, (lane + 1) * cols)
            piece = lax.dot_general(
                gpg, gate_v[span, :], (((1,), (1,)), ((), ())), preferred_element_type=F32
            )
            piece += lax.dot_general(
                gpu, up_v[span, :], (((1,), (1,)), ((), ())), preferred_element_type=F32
            )
            part[lane, rows, :] = piece.astype(BF16)
        first_up(i).start()
        first_dn(i).start()

    def stage_first(i):
        lower, upper = at(i, 0, half), at(i, half, half)
        first_up(i).wait_recv()
        part[up_q, lower, :] = (
            part[up_q, lower, :].astype(F32) + rs1a[i].astype(F32)
        ).astype(BF16)
        last_up(i).start()
        first_dn(i).wait_recv()
        part[dn_q, upper, :] = (
            part[dn_q, upper, :].astype(F32) + rs1b[i].astype(F32)
        ).astype(BF16)
        last_dn(i).start()

    def return_copy(i, k):
        source = ((z - offset(i) + chunks) % chunks) * group + (g + k) % group
        return pltpu.make_async_remote_copy(
            src_ref=ret_src.at[pl.ds(pl.multiple_of(source * cap, cap), cap), :],
            dst_ref=returned.at[own, :],
            send_sem=send_r,
            recv_sem=recv_r,
            device_id=(source, q),
            device_id_type=MESH,
        )

    def stage_return(i):
        rows = at(i)
        last_up(i).wait_recv()
        last_dn(i).wait_recv()
        total = part[q, rows, :].astype(F32) + rs2a[i].astype(F32) + rs2b[i].astype(F32)
        ret_src[rows, :] = total.astype(BF16)

        @pl.when(i > 0)
        def _():
            return_copy(i, 0).start()

        def send_one(k, carry):
            return_copy(i, k).start()
            return carry

        lax.fori_loop(1, group, send_one, 0)

    stages = (stage_gather, stage_pass, stage_compute, stage_first, stage_return)

    def step(t, carry):
        for depth, stage in enumerate(stages):
            i = t - depth

            @pl.when((i >= 0) & (i < chunks))
            def _():
                stage(i)

        return carry

    lax.fori_loop(0, chunks + len(stages) - 1, step, 0)
    returned[own, :] = ret_src[own, :]
    rest = pl.ds(0, (sps - 1) * cap)
    final = pltpu.make_async_remote_copy(
        src_ref=ret_src.at[rest, :],
        dst_ref=returned.at[rest, :],
        send_sem=send_r,
        recv_sem=recv_r,
        device_id=(me, up_q),
        device_id_type=MESH,
    )
    final.wait_recv()

    tokens = grad_input.shape[0]
    own_grad = (
        own_rows[...].astype(F32)
        + jnp.dot(chosen_t[...], returned[...], preferred_element_type=F32)
    ).astype(BF16)
    grad_input[...] = own_grad
    full_in[q] = own_grad

    def share(lane, first, size, kind, peer):
        ref = full_in.at[lane, pl.ds(first, size), :]
        return pltpu.make_async_remote_copy(
            src_ref=ref,
            dst_ref=ref,
            send_sem=send_s.at[kind],
            recv_sem=recv_s.at[kind],
            device_id=(me, peer),
            device_id_type=MESH,
        )

    split = tokens // 2
    shares = (
        share(q, 0, tokens, 0, up_q),
        share(q, 0, tokens, 1, dn_q),
        share(dn_q, 0, split, 2, up_q),
        share(up_q, split, split, 3, dn_q),
    )
    shares[0].start()
    shares[1].start()

    contract0 = (((0,), (0,)), ((), ()))
    per_lane = sps // tps
    owned = g_out.shape[0]

    def send_terms(lane):
        out_terms[lane] = lax.dot_general(
            full_in[lane], mixed[...], contract0, preferred_element_type=F32
        ).astype(BF16)

        def send_one(k, carry):
            place = (g + k) % per_lane
            owner = lane * per_lane + place

            @pl.when(owner != me)
            def _():
                pltpu.make_async_remote_copy(
                    src_ref=out_terms.at[lane, pl.ds(pl.multiple_of(place * owned, owned), owned), :],
                    dst_ref=out_in.at[me],
                    send_sem=send_o,
                    recv_sem=recv_o,
                    device_id=(owner, q),
                    device_id_type=MESH,
                ).start()

            @pl.when(owner == me)
            def _():
                out_in[me] = out_terms[lane, pl.ds(pl.multiple_of(place * owned, owned), owned), :]

            return carry

        lax.fori_loop(0, per_lane, send_one, 0)

    send_terms(q)

    for lane in range(tps):
        span = slice(lane * cols, (lane + 1) * cols)
        g_down[:, span] = lax.dot_general(
            hidden_s[...], routed[lane], contract0, preferred_element_type=F32
        ).astype(BF16)
        g_gate[span, :] = lax.dot_general(
            x_v[:, span], gpg_s[...], contract0, preferred_element_type=F32
        ).astype(BF16)
        g_up[span, :] = lax.dot_general(
            x_v[:, span], gpu_s[...], contract0, preferred_element_type=F32
        ).astype(BF16)

    shares[0].wait_recv()
    shares[2].start()
    shares[1].wait_recv()
    shares[3].start()
    send_terms(dn_q)
    send_terms(up_q)
    shares[2].wait_recv()
    shares[3].wait_recv()
    send_terms(far_q)

    grad_mixed = jnp.zeros((tokens, out_weight.shape[1]), F32)
    for lane in range(tps):
        grad_mixed += jnp.dot(
            full_in[lane],
            out_weight[lane * cols : (lane + 1) * cols, :],
            preferred_element_type=F32,
        )
    sums[0:tokens, :] = grad_mixed * gate_in[...].astype(F32)
    edge = sums.shape[0] - tokens
    shift = pltpu.make_async_remote_copy(
        src_ref=sums.at[pl.ds(0, edge), :],
        dst_ref=sums.at[pl.ds(tokens, edge), :],
        send_sem=send_n,
        recv_sem=recv_n,
        device_id=((me + sps - 1) % sps, q),
        device_id_type=MESH,
    )
    shift.start()
    g_gate_in[...] = (grad_mixed * conv_sum[...].astype(F32)).astype(BF16)
    shift.wait_recv()

    @pl.when(me == sps - 1)
    def _():
        sums[tokens : tokens + edge, :] = jnp.zeros((edge, sums.shape[1]), F32)

    grad_prod = (
        taps[0:1, :] * sums[2 : tokens + 2, :]
        + taps[1:2, :] * sums[1 : tokens + 1, :]
        + taps[2:3, :] * sums[0:tokens, :]
    )
    g_conv_c[...] = (grad_prod * conv_v[...].astype(F32)).astype(BF16)
    g_conv_v[...] = (grad_prod * conv_c[...].astype(F32)).astype(BF16)

    others = out_in.at[pl.ds(0, sps - 1)]
    terms = pltpu.make_async_remote_copy(
        src_ref=others,
        dst_ref=others,
        send_sem=send_o,
        recv_sem=recv_o,
        device_id=(me, up_q),
        device_id_type=MESH,
    )
    terms.wait_recv()
    g_out[...] = jnp.sum(out_in[...].astype(F32), axis=0)

    terms.wait_send()
    shift.wait_send()
    for copy in shares:
        copy.wait_send()

    def drain(i, carry):
        for copy in every:
            copy(i).wait_send()
        return carry

    lax.fori_loop(0, chunks, drain, 0)

    def drain_z(i, count):
        rows = pl.ds(0, count * cap)
        pltpu.make_async_remote_copy(
            src_ref=out_ref.at[rows, :],
            dst_ref=routed.at[q, rows, :],
            send_sem=send_z.at[i],
            recv_sem=recv_z.at[i],
            device_id=(me, up_q),
            device_id_type=MESH,
        ).wait_send()

    drain_z(0, group - 1)

    def drain_rest(i, carry):
        drain_z(i, group)
        return carry

    lax.fori_loop(1, chunks, drain_rest, 0)
    final.wait_send()


def run_step(dims, small, large):
    sps, tps, chunks, cap = dims
    outgoing, chosen, own_rows, out_weight = small[:4]
    gate = large[1]
    rows, cols = outgoing.shape
    tokens = own_rows.shape[0]
    lane_w = out_weight.shape[1]
    width, units = gate.shape
    rows_c = rows // chunks
    vmem = pl.BlockSpec(memory_space=pltpu.VMEM)
    hbm = pl.BlockSpec(memory_space=pltpu.HBM)
    dma = pltpu.SemaphoreType.DMA
    scratch = [
        pltpu.VMEM((rows, cols), BF16),
        pltpu.VMEM((tokens, rows), BF16),
        pltpu.VMEM((tps, tokens, cols), BF16),
        pltpu.VMEM((tokens, lane_w), BF16),
        pltpu.VMEM((tokens + 8, lane_w), F32),
        pltpu.VMEM((tps, cols, lane_w), BF16),
        pltpu.VMEM((sps, width // sps, lane_w), BF16),
        pltpu.VMEM((rows, width), BF16),
        pltpu.VMEM((width, units), BF16),
        pltpu.VMEM((width, units), BF16),
        pltpu.VMEM((units, width), BF16),
        pltpu.VMEM((tps, rows, cols), BF16),
        pltpu.VMEM((tps, rows, cols), BF16),
        pltpu.VMEM((chunks, rows_c // 2, cols), BF16),
        pltpu.VMEM((chunks, rows_c // 2, cols), BF16),
        pltpu.VMEM((chunks, rows_c, cols), BF16),
        pltpu.VMEM((chunks, rows_c, cols), BF16),
        pltpu.VMEM((rows, cols), BF16),
        pltpu.VMEM((rows, units), F32),
        pltpu.VMEM((rows, units), F32),
        pltpu.VMEM((rows, units), BF16),
        pltpu.VMEM((rows, units), BF16),
        pltpu.VMEM((rows, units), BF16),
        dma((4,)),
        dma((chunks,)),
        dma((chunks,)),
        dma((8, chunks)),
        dma((8, chunks)),
        dma,
        dma,
        dma((4,)),
        dma((4,)),
        dma,
        dma,
        dma,
        dma,
    ]
    outs = (
        ((tokens, cols), BF16),
        ((width, units), BF16),
        ((width, units), BF16),
        ((units, width), BF16),
        ((width // sps, lane_w), F32),
        ((tokens, lane_w), BF16),
        ((tokens, lane_w), BF16),
        ((tokens, lane_w), BF16),
    )
    return pl.pallas_call(
        functools.partial(step_kernel, dims),
        out_shape=tuple(jax.ShapeDtypeStruct(*out) for out in outs),
        in_specs=[vmem] * len(small) + [hbm] * len(large),
        out_specs=(vmem,) * len(outs),
        scratch_shapes=scratch,
        compiler_params=pltpu.CompilerParams(
            collective_id=0, has_side_effects=True, vmem_limit_bytes=60 * 1024 * 1024
        ),
        name="step",
    )(*small, *large)


def routing(route_ids, route_weights, experts, capacity):
    tokens = route_ids.shape[0]
    ids = route_ids.T
    weights = route_weights.T
    names = lax.broadcasted_iota(jnp.int32, (experts, tokens), 0)
    first, second = names == ids[0][None, :], names == ids[1][None, :]
    weight = jnp.where(first, weights[0][None, :], 0.0) + jnp.where(
        second, weights[1][None, :], 0.0
    )
    named = first | second
    earlier = lax.broadcasted_iota(jnp.int32, (tokens, tokens), 0) < lax.broadcasted_iota(
        jnp.int32, (tokens, tokens), 1
    )
    rank = jnp.dot(named.astype(BF16), earlier.astype(BF16), preferred_element_type=F32)
    rank = jnp.where(named, rank.astype(jnp.int32), -1)
    slots = lax.broadcasted_iota(jnp.int32, (experts, capacity, tokens), 1)
    chosen = rank[:, None, :] == slots
    slot_weight = jnp.sum(jnp.where(chosen, weight[:, None, :], 0.0), axis=2)
    return chosen.reshape(experts * capacity, tokens).astype(BF16), slot_weight.reshape(-1, 1)


def body(
    chunks,
    cotangent,
    route_ids,
    route_weights,
    expert_inputs,
    gate_weight,
    up_weight,
    down_weight,
    out_weight,
    gate_in,
    conv_sum,
    conv_c,
    conv_v,
    conv_taps,
):
    groups = lax.axis_size("sp")
    lanes = lax.axis_size("tp")
    capacity = expert_inputs.shape[1] // groups
    experts = groups
    model_width = cotangent.shape[1]
    lane_cols = model_width // lanes
    own_rows = lax.dynamic_slice_in_dim(cotangent, lax.axis_index("tp") * lane_cols, lane_cols, 1)
    chosen, slot_weight = routing(route_ids, route_weights, experts, capacity)
    picked = jnp.dot(chosen, own_rows, preferred_element_type=F32)
    outgoing = (slot_weight * picked).astype(BF16)
    grad_input, grad_gate, grad_up, grad_down, *rest = run_step(
        (groups, lanes, chunks, capacity),
        (
            outgoing,
            chosen,
            own_rows,
            out_weight,
            gate_in,
            conv_sum,
            conv_c,
            conv_v,
            conv_taps,
        ),
        (expert_inputs[0], gate_weight[0], up_weight[0], down_weight[0]),
    )
    return (grad_input, grad_gate[None], grad_up[None], grad_down[None], *rest)


def solution(mesh):
    placed = (
        P("sp", None),
        P("sp", None),
        P("sp", None),
        P("sp", None, None),
        P("sp", None, "tp"),
        P("sp", None, "tp"),
        P("sp", "tp", None),
        P(None, "tp"),
        P("sp", "tp"),
        P("sp", "tp"),
        P("sp", "tp"),
        P("sp", "tp"),
        P(None, "tp"),
    )
    chunks = min(8, mesh.shape["sp"] // 2)
    return jax.shard_map(
        functools.partial(body, chunks),
        mesh=mesh,
        in_specs=placed,
        out_specs=(
            P("sp", "tp"),
            P("sp", None, "tp"),
            P("sp", None, "tp"),
            P("sp", "tp", None),
            P("sp", "tp"),
            P("sp", "tp"),
            P("sp", "tp"),
            P("sp", "tp"),
        ),
        check_vma=False,
    )
```

```python
import functools

import jax
import jax.numpy as jnp
from jax import lax
from jax.experimental import pallas as pl
from jax.experimental.pallas import tpu as pltpu
from jax.sharding import PartitionSpec as P

MESH = pl.DeviceIdType.MESH
F32 = jnp.float32
BF16 = jnp.bfloat16


def step_kernel(
    dims,
    ids,
    weights,
    cot,
    out_weight,
    gate_in,
    conv_sum,
    conv_c,
    conv_v,
    taps,
    x_hbm,
    gate_hbm,
    up_hbm,
    down_hbm,
    grad_input,
    g_gate,
    g_up,
    g_down,
    g_out,
    g_gate_in,
    g_conv_c,
    g_conv_v,
    out_ref,
    near_ref,
    chosen,
    slot_weight,
    returned,
    chosen_t,
    full_in,
    mixed,
    sums,
    out_terms,
    out_in,
    x_v,
    gate_v,
    up_v,
    down_v,
    routed,
    part,
    rs1a,
    rs1b,
    rs2a,
    rs2b,
    ret_src,
    swish_s,
    slope_s,
    hidden_s,
    gpg_s,
    gpu_s,
    load_sem,
    send_z,
    recv_z,
    send_y,
    recv_y,
    send_r,
    recv_r,
    send_s,
    recv_s,
    send_o,
    recv_o,
    send_n,
    recv_n,
):
    sps, tps, chunks, cap = dims
    near = 3
    group = sps // chunks
    rows_c = group * cap
    half = rows_c // 2
    cols = out_ref.shape[1]
    tokens = cot.shape[0]
    rows_all = sps * cap
    me = lax.axis_index("sp")
    q = lax.axis_index("tp")
    z = me // group
    g = me % group
    up_q = (q + 1) % tps
    dn_q = (q + tps - 1) % tps
    far_q = (q + 2) % tps

    loads = [
        pltpu.make_async_copy(src, dst, load_sem.at[n])
        for n, (src, dst) in enumerate(
            ((x_hbm, x_v), (gate_hbm, gate_v), (up_hbm, up_v), (down_hbm, down_v))
        )
    ]
    for load in loads:
        load.start()

    barrier = pltpu.get_barrier_semaphore()

    def greet(k, carry):
        pl.semaphore_signal(
            barrier, inc=1, device_id=((me + k) % sps, q), device_id_type=MESH
        )
        return carry

    lax.fori_loop(1, sps, greet, 0)
    for peer in (up_q, dn_q):
        pl.semaphore_signal(barrier, inc=1, device_id=(me, peer), device_id_type=MESH)

    names = lax.broadcasted_iota(jnp.int32, (sps, tokens), 0)
    first, second = names == ids[0:1, :], names == ids[1:2, :]
    weight = jnp.where(first, weights[0:1, :], 0.0) + jnp.where(second, weights[1:2, :], 0.0)
    named = first | second
    earlier = lax.broadcasted_iota(jnp.int32, (tokens, tokens), 0) < lax.broadcasted_iota(
        jnp.int32, (tokens, tokens), 1
    )
    rank = jnp.dot(
        jnp.where(named, 1.0, 0.0).astype(BF16),
        jnp.where(earlier, 1.0, 0.0).astype(BF16),
        preferred_element_type=F32,
    ).astype(jnp.int32)
    rank = jnp.where(named, rank, -1)
    pick = rank[:, None, :] == lax.broadcasted_iota(jnp.int32, (sps, cap, tokens), 1)
    chosen[...] = jnp.where(pick, 1.0, 0.0).reshape(rows_all, tokens).astype(BF16)
    slot_weight[...] = jnp.sum(
        jnp.where(pick, weight[:, None, :], 0.0).reshape(rows_all, tokens), axis=1, keepdims=True
    )
    lane_span = pl.ds(pl.multiple_of(q * cols, cols), cols)
    for slot, step_z in enumerate((0, 1, chunks - 1)):
        rows = pl.ds(pl.multiple_of(((z + step_z) % chunks) * rows_c, rows_c), rows_c)
        near_ref[slot * rows_c : (slot + 1) * rows_c, :] = (
            slot_weight[rows, :]
            * jnp.dot(chosen[rows, :], cot[...], preferred_element_type=F32)
        ).astype(BF16)
    out_ref[...] = (
        slot_weight[...] * jnp.dot(chosen[...], cot[:, lane_span], preferred_element_type=F32)
    ).astype(BF16)
    pl.semaphore_wait(barrier, sps - 1 + 2)

    far_last = chunks - near

    def offset(i):
        u = (i + chunks - 1) % chunks
        w = u // (chunks - 3)
        far = (2 + u // 2) * (1 - 2 * (u % 2))
        return ((i + chunks - 1) // chunks) * (
            (1 - w) * far + w * (1 - 2 * ((u - (chunks - 3)) % 2))
        )

    def chunk_start(i):
        return ((z - offset(i) + chunks) % chunks) * rows_c

    def peer_of(i, k):
        return ((z + offset(i) + chunks) % chunks) * group + (g + k) % group

    own = pl.ds(pl.multiple_of(me * cap, cap), cap)

    def near_copy(i, slot, k):
        row = slot * rows_c + ((g + k) % group) * cap
        return pltpu.make_async_remote_copy(
            src_ref=near_ref.at[pl.ds(pl.multiple_of(row, cap), cap), :],
            dst_ref=routed.at[own, :],
            send_sem=send_z.at[i],
            recv_sem=recv_z.at[i],
            device_id=(peer_of(i, k), q),
            device_id_type=MESH,
        )

    def far_copy(i, k):
        peer = peer_of(i, k)
        return pltpu.make_async_remote_copy(
            src_ref=out_ref.at[pl.ds(pl.multiple_of(peer * cap, cap), cap), :],
            dst_ref=routed.at[own, lane_span],
            send_sem=send_z.at[i],
            recv_sem=recv_z.at[i],
            device_id=(peer, q),
            device_id_type=MESH,
        )

    def send_own(k, carry):
        near_copy(0, 0, k).start()
        return carry

    def send_far(i, carry):
        def send_one(k, inner):
            far_copy(i, k).start()
            return inner

        return lax.fori_loop(0, group, send_one, carry)

    def send_near(i, carry):
        def send_one(k, inner):
            near_copy(i, i - far_last, k).start()
            return inner

        return lax.fori_loop(0, group, send_one, carry)

    lax.fori_loop(1, group, send_own, 0)
    lax.fori_loop(1, far_last + 1, send_far, 0)
    lax.fori_loop(far_last + 1, chunks, send_near, 0)
    routed[own, :] = near_ref[pl.ds(pl.multiple_of(g * cap, cap), cap), :]

    chosen_t[...] = chosen[...].T
    mixed[...] = (gate_in[...].astype(F32) * conv_sum[...].astype(F32)).astype(BF16)

    for load in loads:
        load.wait()

    def at(i, first=0, size=None):
        return pl.ds(pl.multiple_of(chunk_start(i) + first, half), size or rows_c)

    def forward(i):
        rows = at(i)
        pre_gate = jnp.dot(x_v[rows, :], gate_v[...], preferred_element_type=F32)
        pre_up = jnp.dot(x_v[rows, :], up_v[...], preferred_element_type=F32)
        sig = jax.nn.sigmoid(pre_gate)
        swish = pre_gate * sig
        swish_s[rows, :] = swish
        slope_s[rows, :] = pre_up * sig * (1.0 + pre_gate * (1.0 - sig))
        hidden_s[rows, :] = (swish * pre_up).astype(BF16)

    def y_copy(src, dst, kind, i, peer):
        return pltpu.make_async_remote_copy(
            src_ref=src,
            dst_ref=dst,
            send_sem=send_y.at[kind, i],
            recv_sem=recv_y.at[kind, i],
            device_id=(me, peer),
            device_id_type=MESH,
        )

    def lanes_of(lane):
        return pl.ds(pl.multiple_of(lane * cols, cols), cols)

    def gather_up(i):
        ref = routed.at[at(i), lanes_of(q)]
        return y_copy(ref, ref, 0, i, up_q)

    def gather_dn(i):
        ref = routed.at[at(i), lanes_of(q)]
        return y_copy(ref, ref, 1, i, dn_q)

    def pass_up(i):
        ref = routed.at[at(i, 0, half), lanes_of(dn_q)]
        return y_copy(ref, ref, 2, i, up_q)

    def pass_dn(i):
        ref = routed.at[at(i, half, half), lanes_of(up_q)]
        return y_copy(ref, ref, 3, i, dn_q)

    def first_up(i):
        return y_copy(part.at[far_q, at(i, 0, half), :], rs1a.at[i], 4, i, up_q)

    def first_dn(i):
        return y_copy(part.at[far_q, at(i, half, half), :], rs1b.at[i], 5, i, dn_q)

    def last_up(i):
        return y_copy(part.at[up_q, at(i), :], rs2a.at[i], 6, i, up_q)

    def last_dn(i):
        return y_copy(part.at[dn_q, at(i), :], rs2b.at[i], 7, i, dn_q)

    every = (gather_up, gather_dn, pass_up, pass_dn, first_up, first_dn, last_up, last_dn)

    def far_block(i):
        return pltpu.make_async_remote_copy(
            src_ref=out_ref.at[pl.ds(0, rows_c), :],
            dst_ref=routed.at[pl.ds(0, rows_c), lane_span],
            send_sem=send_z.at[i],
            recv_sem=recv_z.at[i],
            device_id=(me, up_q),
            device_id_type=MESH,
        )

    def near_block(i, count):
        rows = pl.ds(0, count * cap)
        return pltpu.make_async_remote_copy(
            src_ref=near_ref.at[rows, :],
            dst_ref=routed.at[rows, :],
            send_sem=send_z.at[i],
            recv_sem=recv_z.at[i],
            device_id=(me, up_q),
            device_id_type=MESH,
        )

    def stage_gather(i):
        far_block(i).wait_recv()
        gather_up(i).start()
        gather_dn(i).start()

    def stage_pass(i):
        gather_up(i).wait_recv()
        pass_up(i).start()
        gather_dn(i).wait_recv()
        pass_dn(i).start()

    def compute(i):
        rows = at(i)
        grad_hidden = jnp.zeros((rows_c, down_v.shape[0]), F32)
        for lane in range(tps):
            grad_hidden += lax.dot_general(
                routed[rows, lane * cols : (lane + 1) * cols],
                down_v[:, lane * cols : (lane + 1) * cols],
                (((1,), (1,)), ((), ())),
                preferred_element_type=F32,
            )
        gpg = (grad_hidden * slope_s[rows, :]).astype(BF16)
        gpu = (grad_hidden * swish_s[rows, :]).astype(BF16)
        gpg_s[rows, :] = gpg
        gpu_s[rows, :] = gpu
        for lane in range(tps):
            span = slice(lane * cols, (lane + 1) * cols)
            piece = lax.dot_general(
                gpg, gate_v[span, :], (((1,), (1,)), ((), ())), preferred_element_type=F32
            )
            piece += lax.dot_general(
                gpu, up_v[span, :], (((1,), (1,)), ((), ())), preferred_element_type=F32
            )
            part[lane, rows, :] = piece.astype(BF16)
        first_up(i).start()
        first_dn(i).start()

    def stage_compute(i):
        @pl.when(i <= far_last)
        def _():
            pass_up(i).wait_recv()
            pass_dn(i).wait_recv()

        @pl.when(i > far_last)
        def _():
            near_block(i, group).wait_recv()

        compute(i)

    def stage_first(i):
        lower, upper = at(i, 0, half), at(i, half, half)
        first_up(i).wait_recv()
        part[up_q, lower, :] = (
            part[up_q, lower, :].astype(F32) + rs1a[i].astype(F32)
        ).astype(BF16)
        last_up(i).start()
        first_dn(i).wait_recv()
        part[dn_q, upper, :] = (
            part[dn_q, upper, :].astype(F32) + rs1b[i].astype(F32)
        ).astype(BF16)
        last_dn(i).start()

    def return_copy(i, k):
        source = ((z - offset(i) + chunks) % chunks) * group + (g + k) % group
        return pltpu.make_async_remote_copy(
            src_ref=ret_src.at[pl.ds(pl.multiple_of(source * cap, cap), cap), :],
            dst_ref=returned.at[own, :],
            send_sem=send_r,
            recv_sem=recv_r,
            device_id=(source, q),
            device_id_type=MESH,
        )

    def stage_return(i):
        rows = at(i)
        last_up(i).wait_recv()
        last_dn(i).wait_recv()
        total = part[q, rows, :].astype(F32) + rs2a[i].astype(F32) + rs2b[i].astype(F32)
        ret_src[rows, :] = total.astype(BF16)

        @pl.when(i > 0)
        def _():
            return_copy(i, 0).start()

        def send_one(k, carry):
            return_copy(i, k).start()
            return carry

        lax.fori_loop(1, group, send_one, 0)

    forward(0)
    if group > 1:
        near_block(0, group - 1).wait_recv()
    compute(0)
    forward(1)
    stage_first(0)

    def step(t, carry):
        for stage, lead, first, last in (
            (stage_gather, 1, 1, far_last),
            (stage_pass, 0, 1, far_last),
            (stage_compute, -1, 1, chunks - 1),
            (forward, 2, 2, chunks - 1),
            (stage_first, -2, 1, chunks - 1),
            (stage_return, -3, 0, chunks - 1),
        ):
            i = t + lead

            @pl.when((i >= first) & (i <= last))
            def _():
                stage(i)

        return carry

    lax.fori_loop(0, chunks + 3, step, 0)
    returned[own, :] = ret_src[own, :]
    rest = pl.ds(0, (sps - 1) * cap)
    final = pltpu.make_async_remote_copy(
        src_ref=ret_src.at[rest, :],
        dst_ref=returned.at[rest, :],
        send_sem=send_r,
        recv_sem=recv_r,
        device_id=(me, up_q),
        device_id_type=MESH,
    )
    final.wait_recv()

    own_grad = (
        cot[:, lane_span].astype(F32)
        + jnp.dot(chosen_t[...], returned[...], preferred_element_type=F32)
    ).astype(BF16)
    grad_input[...] = own_grad
    full_in[q] = own_grad

    def share(lane, first, size, kind, peer):
        ref = full_in.at[lane, pl.ds(first, size), :]
        return pltpu.make_async_remote_copy(
            src_ref=ref,
            dst_ref=ref,
            send_sem=send_s.at[kind],
            recv_sem=recv_s.at[kind],
            device_id=(me, peer),
            device_id_type=MESH,
        )

    split = tokens // 2
    shares = (
        share(q, 0, tokens, 0, up_q),
        share(q, 0, tokens, 1, dn_q),
        share(dn_q, 0, split, 2, up_q),
        share(up_q, split, split, 3, dn_q),
    )
    shares[0].start()
    shares[1].start()

    contract0 = (((0,), (0,)), ((), ()))
    per_lane = sps // tps
    owned = g_out.shape[0]

    def send_terms(lane):
        out_terms[lane] = lax.dot_general(
            full_in[lane], mixed[...], contract0, preferred_element_type=F32
        ).astype(BF16)

        def send_one(k, carry):
            place = (g + k) % per_lane
            owner = lane * per_lane + place

            @pl.when(owner != me)
            def _():
                pltpu.make_async_remote_copy(
                    src_ref=out_terms.at[lane, pl.ds(pl.multiple_of(place * owned, owned), owned), :],
                    dst_ref=out_in.at[me],
                    send_sem=send_o,
                    recv_sem=recv_o,
                    device_id=(owner, q),
                    device_id_type=MESH,
                ).start()

            @pl.when(owner == me)
            def _():
                out_in[me] = out_terms[lane, pl.ds(pl.multiple_of(place * owned, owned), owned), :]

            return carry

        lax.fori_loop(0, per_lane, send_one, 0)

    send_terms(q)

    for lane in range(tps):
        span = slice(lane * cols, (lane + 1) * cols)
        g_down[:, span] = lax.dot_general(
            hidden_s[...], routed[:, span], contract0, preferred_element_type=F32
        ).astype(BF16)
        g_gate[span, :] = lax.dot_general(
            x_v[:, span], gpg_s[...], contract0, preferred_element_type=F32
        ).astype(BF16)
        g_up[span, :] = lax.dot_general(
            x_v[:, span], gpu_s[...], contract0, preferred_element_type=F32
        ).astype(BF16)

    shares[0].wait_recv()
    shares[2].start()
    shares[1].wait_recv()
    shares[3].start()
    send_terms(dn_q)
    send_terms(up_q)
    shares[2].wait_recv()
    shares[3].wait_recv()
    send_terms(far_q)

    grad_mixed = jnp.zeros((tokens, out_weight.shape[1]), F32)
    for lane in range(tps):
        grad_mixed += jnp.dot(
            full_in[lane],
            out_weight[lane * cols : (lane + 1) * cols, :],
            preferred_element_type=F32,
        )
    sums[0:tokens, :] = grad_mixed * gate_in[...].astype(F32)
    edge = sums.shape[0] - tokens
    shift = pltpu.make_async_remote_copy(
        src_ref=sums.at[pl.ds(0, edge), :],
        dst_ref=sums.at[pl.ds(tokens, edge), :],
        send_sem=send_n,
        recv_sem=recv_n,
        device_id=((me + sps - 1) % sps, q),
        device_id_type=MESH,
    )
    shift.start()
    g_gate_in[...] = (grad_mixed * conv_sum[...].astype(F32)).astype(BF16)
    shift.wait_recv()

    @pl.when(me == sps - 1)
    def _():
        sums[tokens : tokens + edge, :] = jnp.zeros((edge, sums.shape[1]), F32)

    grad_prod = (
        taps[0:1, :] * sums[2 : tokens + 2, :]
        + taps[1:2, :] * sums[1 : tokens + 1, :]
        + taps[2:3, :] * sums[0:tokens, :]
    )
    g_conv_c[...] = (grad_prod * conv_v[...].astype(F32)).astype(BF16)
    g_conv_v[...] = (grad_prod * conv_c[...].astype(F32)).astype(BF16)

    others = out_in.at[pl.ds(0, sps - 1)]
    terms = pltpu.make_async_remote_copy(
        src_ref=others,
        dst_ref=others,
        send_sem=send_o,
        recv_sem=recv_o,
        device_id=(me, up_q),
        device_id_type=MESH,
    )
    terms.wait_recv()
    g_out[...] = jnp.sum(out_in[...].astype(F32), axis=0)

    terms.wait_send()
    shift.wait_send()
    for copy in shares:
        copy.wait_send()

    def drain_far(i, carry):
        for copy in every[:4]:
            copy(i).wait_send()
        far_block(i).wait_send()
        return carry

    def drain_sum(i, carry):
        for copy in every[4:]:
            copy(i).wait_send()
        return carry

    def drain_near(i, carry):
        near_block(i, group).wait_send()
        return carry

    lax.fori_loop(1, far_last + 1, drain_far, 0)
    lax.fori_loop(0, chunks, drain_sum, 0)
    lax.fori_loop(far_last + 1, chunks, drain_near, 0)
    if group > 1:
        near_block(0, group - 1).wait_send()
    final.wait_send()


def run_step(dims, small, large):
    sps, tps, chunks, cap = dims
    cot, out_weight = small[2:4]
    gate = large[1]
    rows = sps * cap
    tokens = cot.shape[0]
    cols = cot.shape[1] // tps
    lane_w = out_weight.shape[1]
    width, units = gate.shape
    rows_c = rows // chunks
    vmem = pl.BlockSpec(memory_space=pltpu.VMEM)
    hbm = pl.BlockSpec(memory_space=pltpu.HBM)
    dma = pltpu.SemaphoreType.DMA
    scratch = [
        pltpu.VMEM((rows, cols), BF16),
        pltpu.VMEM((3 * rows_c, width), BF16),
        pltpu.VMEM((rows, tokens), BF16),
        pltpu.VMEM((rows, 1), F32),
        pltpu.VMEM((rows, cols), BF16),
        pltpu.VMEM((tokens, rows), BF16),
        pltpu.VMEM((tps, tokens, cols), BF16),
        pltpu.VMEM((tokens, lane_w), BF16),
        pltpu.VMEM((tokens + 8, lane_w), F32),
        pltpu.VMEM((tps, cols, lane_w), BF16),
        pltpu.VMEM((sps, width // sps, lane_w), BF16),
        pltpu.VMEM((rows, width), BF16),
        pltpu.VMEM((width, units), BF16),
        pltpu.VMEM((width, units), BF16),
        pltpu.VMEM((units, width), BF16),
        pltpu.VMEM((rows, width), BF16),
        pltpu.VMEM((tps, rows, cols), BF16),
        pltpu.VMEM((chunks, rows_c // 2, cols), BF16),
        pltpu.VMEM((chunks, rows_c // 2, cols), BF16),
        pltpu.VMEM((chunks, rows_c, cols), BF16),
        pltpu.VMEM((chunks, rows_c, cols), BF16),
        pltpu.VMEM((rows, cols), BF16),
        pltpu.VMEM((rows, units), F32),
        pltpu.VMEM((rows, units), F32),
        pltpu.VMEM((rows, units), BF16),
        pltpu.VMEM((rows, units), BF16),
        pltpu.VMEM((rows, units), BF16),
        dma((4,)),
        dma((chunks,)),
        dma((chunks,)),
        dma((8, chunks)),
        dma((8, chunks)),
        dma,
        dma,
        dma((4,)),
        dma((4,)),
        dma,
        dma,
        dma,
        dma,
    ]
    outs = (
        ((tokens, cols), BF16),
        ((width, units), BF16),
        ((width, units), BF16),
        ((units, width), BF16),
        ((width // sps, lane_w), F32),
        ((tokens, lane_w), BF16),
        ((tokens, lane_w), BF16),
        ((tokens, lane_w), BF16),
    )
    return pl.pallas_call(
        functools.partial(step_kernel, dims),
        out_shape=tuple(jax.ShapeDtypeStruct(*out) for out in outs),
        in_specs=[vmem] * len(small) + [hbm] * len(large),
        out_specs=(vmem,) * len(outs),
        scratch_shapes=scratch,
        compiler_params=pltpu.CompilerParams(
            collective_id=0, has_side_effects=True, vmem_limit_bytes=60 * 1024 * 1024
        ),
        name="step",
    )(*small, *large)


def store_kernel(count, *refs):
    sems = refs[-1]
    copies = [
        pltpu.make_async_copy(refs[n], refs[count + n], sems.at[n]) for n in range(count)
    ]
    for copy in copies:
        copy.start()
    for copy in copies:
        copy.wait()


def store(values):
    count = len(values)
    return pl.pallas_call(
        functools.partial(store_kernel, count),
        out_shape=tuple(jax.ShapeDtypeStruct(v.shape, v.dtype) for v in values),
        in_specs=[pl.BlockSpec(memory_space=pltpu.VMEM)] * count,
        out_specs=(pl.BlockSpec(memory_space=pltpu.HBM),) * count,
        scratch_shapes=[pltpu.SemaphoreType.DMA((count,))],
        name="store",
    )(*values)


def body(
    chunks,
    cotangent,
    route_ids,
    route_weights,
    expert_inputs,
    gate_weight,
    up_weight,
    down_weight,
    out_weight,
    gate_in,
    conv_sum,
    conv_c,
    conv_v,
    conv_taps,
):
    groups = lax.axis_size("sp")
    lanes = lax.axis_size("tp")
    capacity = expert_inputs.shape[1] // groups
    results = run_step(
        (groups, lanes, chunks, capacity),
        (
            route_ids.T,
            route_weights.T,
            cotangent,
            out_weight,
            gate_in,
            conv_sum,
            conv_c,
            conv_v,
            conv_taps,
        ),
        (expert_inputs[0], gate_weight[0], up_weight[0], down_weight[0]),
    )
    grad_input, grad_gate, grad_up, grad_down, *rest = store(results)
    return (grad_input, grad_gate[None], grad_up[None], grad_down[None], *rest)


def solution(mesh):
    placed = (
        P("sp", None),
        P("sp", None),
        P("sp", None),
        P("sp", None, None),
        P("sp", None, "tp"),
        P("sp", None, "tp"),
        P("sp", "tp", None),
        P(None, "tp"),
        P("sp", "tp"),
        P("sp", "tp"),
        P("sp", "tp"),
        P("sp", "tp"),
        P(None, "tp"),
    )
    chunks = 8
    return jax.shard_map(
        functools.partial(body, chunks),
        mesh=mesh,
        in_specs=placed,
        out_specs=(
            P("sp", "tp"),
            P("sp", None, "tp"),
            P("sp", None, "tp"),
            P("sp", "tp", None),
            P("sp", "tp"),
            P("sp", "tp"),
            P("sp", "tp"),
            P("sp", "tp"),
        ),
        check_vma=False,
    )
```

```python
import functools

import jax
import jax.numpy as jnp
from jax import lax
from jax.experimental import pallas as pl
from jax.experimental.pallas import tpu as pltpu
from jax.sharding import PartitionSpec as P

MESH = pl.DeviceIdType.MESH
F32 = jnp.float32
BF16 = jnp.bfloat16


def step_kernel(
    dims,
    ids,
    weights,
    cot,
    out_weight,
    gate_in,
    conv_sum,
    conv_c,
    conv_v,
    taps,
    x_hbm,
    gate_hbm,
    up_hbm,
    down_hbm,
    grad_input,
    g_gate_hbm,
    g_up_hbm,
    g_down_hbm,
    g_out,
    g_gate_in,
    g_conv_c,
    g_conv_v,
    out_ref,
    near_ref,
    chosen,
    slot_weight,
    returned,
    chosen_t,
    full_in,
    mixed,
    sums,
    out_terms,
    out_in,
    g_gate,
    g_up,
    g_down,
    x_v,
    gate_v,
    up_v,
    down_v,
    routed,
    part,
    rs1a,
    rs1b,
    rs2a,
    rs2b,
    ret_src,
    swish_s,
    slope_s,
    hidden_s,
    gpg_s,
    gpu_s,
    load_sem,
    store_sem,
    send_z,
    recv_z,
    send_y,
    recv_y,
    send_r,
    recv_r,
    send_s,
    recv_s,
    send_o,
    recv_o,
    send_n,
    recv_n,
):
    sps, tps, chunks, cap = dims
    near = 3
    group = sps // chunks
    rows_c = group * cap
    half = rows_c // 2
    cols = out_ref.shape[1]
    tokens = cot.shape[0]
    rows_all = sps * cap
    me = lax.axis_index("sp")
    q = lax.axis_index("tp")
    z = me // group
    g = me % group
    up_q = (q + 1) % tps
    dn_q = (q + tps - 1) % tps
    far_q = (q + 2) % tps

    loads = [
        pltpu.make_async_copy(src, dst, load_sem.at[n])
        for n, (src, dst) in enumerate(
            ((x_hbm, x_v), (gate_hbm, gate_v), (up_hbm, up_v), (down_hbm, down_v))
        )
    ]
    for load in loads:
        load.start()

    barrier = pltpu.get_barrier_semaphore()

    def greet(k, carry):
        pl.semaphore_signal(
            barrier, inc=1, device_id=((me + k) % sps, q), device_id_type=MESH
        )
        return carry

    lax.fori_loop(1, sps, greet, 0)
    for peer in (up_q, dn_q):
        pl.semaphore_signal(barrier, inc=1, device_id=(me, peer), device_id_type=MESH)

    names = lax.broadcasted_iota(jnp.int32, (sps, tokens), 0)
    first, second = names == ids[0:1, :], names == ids[1:2, :]
    weight = jnp.where(first, weights[0:1, :], 0.0) + jnp.where(second, weights[1:2, :], 0.0)
    named = first | second
    earlier = lax.broadcasted_iota(jnp.int32, (tokens, tokens), 0) < lax.broadcasted_iota(
        jnp.int32, (tokens, tokens), 1
    )
    rank = jnp.dot(
        jnp.where(named, 1.0, 0.0).astype(BF16),
        jnp.where(earlier, 1.0, 0.0).astype(BF16),
        preferred_element_type=F32,
    ).astype(jnp.int32)
    rank = jnp.where(named, rank, -1)
    pick = rank[:, None, :] == lax.broadcasted_iota(jnp.int32, (sps, cap, tokens), 1)
    chosen[...] = jnp.where(pick, 1.0, 0.0).reshape(rows_all, tokens).astype(BF16)
    slot_weight[...] = jnp.sum(
        jnp.where(pick, weight[:, None, :], 0.0).reshape(rows_all, tokens), axis=1, keepdims=True
    )
    lane_span = pl.ds(pl.multiple_of(q * cols, cols), cols)

    def build_near(slot, step_z):
        rows = pl.ds(pl.multiple_of(((z + step_z) % chunks) * rows_c, rows_c), rows_c)
        near_ref[slot * rows_c : (slot + 1) * rows_c, :] = (
            slot_weight[rows, :]
            * jnp.dot(chosen[rows, :], cot[...], preferred_element_type=F32)
        ).astype(BF16)

    build_near(0, 0)
    pl.semaphore_wait(barrier, sps - 1 + 2)

    far_last = chunks - near

    def offset(i):
        u = (i + chunks - 1) % chunks
        w = u // (chunks - 3)
        far = (2 + u // 2) * (1 - 2 * (u % 2))
        return ((i + chunks - 1) // chunks) * (
            (1 - w) * far + w * (1 - 2 * ((u - (chunks - 3)) % 2))
        )

    def chunk_start(i):
        return ((z - offset(i) + chunks) % chunks) * rows_c

    def peer_of(i, k):
        return ((z + offset(i) + chunks) % chunks) * group + (g + k) % group

    own = pl.ds(pl.multiple_of(me * cap, cap), cap)

    def near_copy(i, slot, k):
        row = slot * rows_c + ((g + k) % group) * cap
        return pltpu.make_async_remote_copy(
            src_ref=near_ref.at[pl.ds(pl.multiple_of(row, cap), cap), :],
            dst_ref=routed.at[own, :],
            send_sem=send_z.at[i],
            recv_sem=recv_z.at[i],
            device_id=(peer_of(i, k), q),
            device_id_type=MESH,
        )

    def far_copy(i, k):
        peer = peer_of(i, k)
        return pltpu.make_async_remote_copy(
            src_ref=out_ref.at[pl.ds(pl.multiple_of(peer * cap, cap), cap), :],
            dst_ref=routed.at[own, lane_span],
            send_sem=send_z.at[i],
            recv_sem=recv_z.at[i],
            device_id=(peer, q),
            device_id_type=MESH,
        )

    def send_own(k, carry):
        near_copy(0, 0, k).start()
        return carry

    def send_far(i, carry):
        def send_one(k, inner):
            far_copy(i, k).start()
            return inner

        return lax.fori_loop(0, group, send_one, carry)

    def send_near(i, carry):
        def send_one(k, inner):
            near_copy(i, i - far_last, k).start()
            return inner

        return lax.fori_loop(0, group, send_one, carry)

    lax.fori_loop(1, group, send_own, 0)
    out_ref[...] = (
        slot_weight[...] * jnp.dot(chosen[...], cot[:, lane_span], preferred_element_type=F32)
    ).astype(BF16)
    lax.fori_loop(1, 3+1, send_far, 0)
    build_near(1, 1)
    build_near(2, chunks - 1)
    routed[own, :] = near_ref[pl.ds(pl.multiple_of(g * cap, cap), cap), :]

    chosen_t[...] = chosen[...].T
    mixed[...] = (gate_in[...].astype(F32) * conv_sum[...].astype(F32)).astype(BF16)

    for load in loads:
        load.wait()

    def at(i, first=0, size=None):
        return pl.ds(pl.multiple_of(chunk_start(i) + first, half), size or rows_c)

    def forward(i):
        rows = at(i)
        pre_gate = jnp.dot(x_v[rows, :], gate_v[...], preferred_element_type=F32)
        pre_up = jnp.dot(x_v[rows, :], up_v[...], preferred_element_type=F32)
        sig = jax.nn.sigmoid(pre_gate)
        swish = pre_gate * sig
        swish_s[rows, :] = swish
        slope_s[rows, :] = pre_up * sig * (1.0 + pre_gate * (1.0 - sig))
        hidden_s[rows, :] = (swish * pre_up).astype(BF16)

    def y_copy(src, dst, kind, i, peer):
        return pltpu.make_async_remote_copy(
            src_ref=src,
            dst_ref=dst,
            send_sem=send_y.at[kind, i],
            recv_sem=recv_y.at[kind, i],
            device_id=(me, peer),
            device_id_type=MESH,
        )

    def lanes_of(lane):
        return pl.ds(pl.multiple_of(lane * cols, cols), cols)

    def gather_up(i):
        ref = routed.at[at(i), lanes_of(q)]
        return y_copy(ref, ref, 0, i, up_q)

    def gather_dn(i):
        ref = routed.at[at(i), lanes_of(q)]
        return y_copy(ref, ref, 1, i, dn_q)

    def pass_up(i):
        ref = routed.at[at(i, 0, half), lanes_of(dn_q)]
        return y_copy(ref, ref, 2, i, up_q)

    def pass_dn(i):
        ref = routed.at[at(i, half, half), lanes_of(up_q)]
        return y_copy(ref, ref, 3, i, dn_q)

    def first_up(i):
        return y_copy(part.at[far_q, at(i, 0, half), :], rs1a.at[i], 4, i, up_q)

    def first_dn(i):
        return y_copy(part.at[far_q, at(i, half, half), :], rs1b.at[i], 5, i, dn_q)

    def last_up(i):
        return y_copy(part.at[up_q, at(i), :], rs2a.at[i], 6, i, up_q)

    def last_dn(i):
        return y_copy(part.at[dn_q, at(i), :], rs2b.at[i], 7, i, dn_q)

    every = (gather_up, gather_dn, pass_up, pass_dn, first_up, first_dn, last_up, last_dn)

    def far_block(i):
        return pltpu.make_async_remote_copy(
            src_ref=out_ref.at[pl.ds(0, rows_c), :],
            dst_ref=routed.at[pl.ds(0, rows_c), lane_span],
            send_sem=send_z.at[i],
            recv_sem=recv_z.at[i],
            device_id=(me, up_q),
            device_id_type=MESH,
        )

    def near_block(i, count):
        rows = pl.ds(0, count * cap)
        return pltpu.make_async_remote_copy(
            src_ref=near_ref.at[rows, :],
            dst_ref=routed.at[rows, :],
            send_sem=send_z.at[i],
            recv_sem=recv_z.at[i],
            device_id=(me, up_q),
            device_id_type=MESH,
        )

    def stage_gather(i):
        far_block(i).wait_recv()
        gather_up(i).start()
        gather_dn(i).start()

        @pl.when(i + 3 <= far_last)
        def _():
            send_far(i + 3, 0)

        @pl.when((i + 3 > far_last) & (i + 3 < chunks))
        def _():
            send_near(i + 3, 0)

    def stage_pass(i):
        gather_up(i).wait_recv()
        pass_up(i).start()
        gather_dn(i).wait_recv()
        pass_dn(i).start()

    def compute(i):
        rows = at(i)
        grad_hidden = jnp.zeros((rows_c, down_v.shape[0]), F32)
        for lane in range(tps):
            grad_hidden += lax.dot_general(
                routed[rows, lane * cols : (lane + 1) * cols],
                down_v[:, lane * cols : (lane + 1) * cols],
                (((1,), (1,)), ((), ())),
                preferred_element_type=F32,
            )
        gpg = (grad_hidden * slope_s[rows, :]).astype(BF16)
        gpu = (grad_hidden * swish_s[rows, :]).astype(BF16)
        gpg_s[rows, :] = gpg
        gpu_s[rows, :] = gpu
        for lane in range(tps):
            span = slice(lane * cols, (lane + 1) * cols)
            piece = lax.dot_general(
                gpg, gate_v[span, :], (((1,), (1,)), ((), ())), preferred_element_type=F32
            )
            piece += lax.dot_general(
                gpu, up_v[span, :], (((1,), (1,)), ((), ())), preferred_element_type=F32
            )
            part[lane, rows, :] = piece.astype(BF16)
        first_up(i).start()
        first_dn(i).start()

    def stage_compute(i):
        @pl.when(i <= far_last)
        def _():
            pass_up(i).wait_recv()
            pass_dn(i).wait_recv()

        @pl.when(i > far_last)
        def _():
            near_block(i, group).wait_recv()

        compute(i)

    def stage_first(i):
        lower, upper = at(i, 0, half), at(i, half, half)
        first_up(i).wait_recv()
        part[up_q, lower, :] = (
            part[up_q, lower, :].astype(F32) + rs1a[i].astype(F32)
        ).astype(BF16)
        last_up(i).start()
        first_dn(i).wait_recv()
        part[dn_q, upper, :] = (
            part[dn_q, upper, :].astype(F32) + rs1b[i].astype(F32)
        ).astype(BF16)
        last_dn(i).start()

    def return_copy(i, k):
        source = ((z - offset(i) + chunks) % chunks) * group + (g + k) % group
        return pltpu.make_async_remote_copy(
            src_ref=ret_src.at[pl.ds(pl.multiple_of(source * cap, cap), cap), :],
            dst_ref=returned.at[own, :],
            send_sem=send_r,
            recv_sem=recv_r,
            device_id=(source, q),
            device_id_type=MESH,
        )

    def stage_return(i):
        rows = at(i)
        last_up(i).wait_recv()
        last_dn(i).wait_recv()
        total = part[q, rows, :].astype(F32) + rs2a[i].astype(F32) + rs2b[i].astype(F32)
        ret_src[rows, :] = total.astype(BF16)

        @pl.when(i > 0)
        def _():
            return_copy(i, 0).start()

        def send_one(k, carry):
            return_copy(i, k).start()
            return carry

        lax.fori_loop(1, group, send_one, 0)

    forward(0)
    if group > 1:
        near_block(0, group - 1).wait_recv()
    compute(0)
    forward(1)
    stage_first(0)

    def step(t, carry):
        for stage, lead, first, last in (
            (stage_gather, 1, 1, far_last),
            (stage_pass, 0, 1, far_last),
            (stage_compute, -1, 1, chunks - 1),
            (forward, 2, 2, chunks - 1),
            (stage_first, -2, 1, chunks - 1),
            (stage_return, -3, 0, chunks - 1),
        ):
            i = t + lead

            @pl.when((i >= first) & (i <= last))
            def _():
                stage(i)

        return carry

    lax.fori_loop(0, chunks + 3, step, 0)
    returned[own, :] = ret_src[own, :]
    rest = pl.ds(0, (sps - 1) * cap)
    final = pltpu.make_async_remote_copy(
        src_ref=ret_src.at[rest, :],
        dst_ref=returned.at[rest, :],
        send_sem=send_r,
        recv_sem=recv_r,
        device_id=(me, up_q),
        device_id_type=MESH,
    )
    contract0 = (((0,), (0,)), ((), ()))
    stores = [
        pltpu.make_async_copy(src, dst, store_sem.at[n])
        for n, (src, dst) in enumerate(
            ((g_down, g_down_hbm), (g_gate, g_gate_hbm), (g_up, g_up_hbm))
        )
    ]
    for lane in range(tps):
        span = slice(lane * cols, (lane + 1) * cols)
        g_down[:, span] = lax.dot_general(
            hidden_s[...], routed[:, span], contract0, preferred_element_type=F32
        ).astype(BF16)
    stores[0].start()
    for lane in range(tps):
        span = slice(lane * cols, (lane + 1) * cols)
        g_gate[span, :] = lax.dot_general(
            x_v[:, span], gpg_s[...], contract0, preferred_element_type=F32
        ).astype(BF16)
    stores[1].start()
    final.wait_recv()

    pieces = 2
    wide = cols // pieces
    split = tokens // 2

    def share(lane, piece, first, size, kind, peer):
        ref = full_in.at[lane, pl.ds(first, size), pl.ds(piece * wide, wide)]
        return pltpu.make_async_remote_copy(
            src_ref=ref,
            dst_ref=ref,
            send_sem=send_s.at[kind, piece],
            recv_sem=recv_s.at[kind, piece],
            device_id=(me, peer),
            device_id_type=MESH,
        )

    shares = [
        (
            share(q, piece, 0, tokens, 0, up_q),
            share(q, piece, 0, tokens, 1, dn_q),
            share(dn_q, piece, 0, split, 2, up_q),
            share(up_q, piece, split, split, 3, dn_q),
        )
        for piece in range(pieces)
    ]
    per_lane = sps // tps
    per_piece = per_lane // pieces
    owned = g_out.shape[0]

    def send_terms(lane, piece):
        span = slice(piece * wide, (piece + 1) * wide)
        out_terms[lane, span, :] = lax.dot_general(
            full_in[lane, :, span], mixed[...], contract0, preferred_element_type=F32
        ).astype(BF16)

        def send_one(k, carry):
            place = piece * per_piece + (g + k) % per_piece
            owner = lane * per_lane + place
            block = pl.ds(pl.multiple_of(place * owned, owned), owned)

            @pl.when(owner != me)
            def _():
                pltpu.make_async_remote_copy(
                    src_ref=out_terms.at[lane, block, :],
                    dst_ref=out_in.at[me],
                    send_sem=send_o,
                    recv_sem=recv_o,
                    device_id=(owner, q),
                    device_id_type=MESH,
                ).start()

            @pl.when(owner == me)
            def _():
                out_in[me] = out_terms[lane, block, :]

            return carry

        lax.fori_loop(0, per_piece, send_one, 0)

    for piece in range(pieces):
        span = slice(piece * wide, (piece + 1) * wide)
        own_cols = pl.ds(pl.multiple_of(q * cols + piece * wide, wide), wide)
        own_grad = (
            cot[:, own_cols].astype(F32)
            + jnp.dot(chosen_t[...], returned[:, span], preferred_element_type=F32)
        ).astype(BF16)
        grad_input[:, span] = own_grad
        full_in[q, :, span] = own_grad
        shares[piece][0].start()
        shares[piece][1].start()
    for piece in range(pieces):
        send_terms(q, piece)
    for lane in range(tps):
        span = slice(lane * cols, (lane + 1) * cols)
        g_up[span, :] = lax.dot_general(
            x_v[:, span], gpu_s[...], contract0, preferred_element_type=F32
        ).astype(BF16)
    stores[2].start()

    for piece in range(pieces):
        shares[piece][0].wait_recv()
        shares[piece][2].start()
        shares[piece][1].wait_recv()
        shares[piece][3].start()
        send_terms(dn_q, piece)
        send_terms(up_q, piece)
    for piece in range(pieces):
        shares[piece][2].wait_recv()
        shares[piece][3].wait_recv()
        send_terms(far_q, piece)

    grad_mixed = jnp.zeros((tokens, out_weight.shape[1]), F32)
    for lane in range(tps):
        grad_mixed += jnp.dot(
            full_in[lane],
            out_weight[lane * cols : (lane + 1) * cols, :],
            preferred_element_type=F32,
        )
    sums[0:tokens, :] = grad_mixed * gate_in[...].astype(F32)
    edge = sums.shape[0] - tokens
    shift = pltpu.make_async_remote_copy(
        src_ref=sums.at[pl.ds(0, edge), :],
        dst_ref=sums.at[pl.ds(tokens, edge), :],
        send_sem=send_n,
        recv_sem=recv_n,
        device_id=((me + sps - 1) % sps, q),
        device_id_type=MESH,
    )
    shift.start()
    g_gate_in[...] = (grad_mixed * conv_sum[...].astype(F32)).astype(BF16)
    shift.wait_recv()

    @pl.when(me == sps - 1)
    def _():
        sums[tokens : tokens + edge, :] = jnp.zeros((edge, sums.shape[1]), F32)

    grad_prod = (
        taps[0:1, :] * sums[2 : tokens + 2, :]
        + taps[1:2, :] * sums[1 : tokens + 1, :]
        + taps[2:3, :] * sums[0:tokens, :]
    )
    g_conv_c[...] = (grad_prod * conv_v[...].astype(F32)).astype(BF16)
    g_conv_v[...] = (grad_prod * conv_c[...].astype(F32)).astype(BF16)

    others = out_in.at[pl.ds(0, sps - 1)]
    terms = pltpu.make_async_remote_copy(
        src_ref=others,
        dst_ref=others,
        send_sem=send_o,
        recv_sem=recv_o,
        device_id=(me, up_q),
        device_id_type=MESH,
    )
    terms.wait_recv()
    g_out[...] = jnp.sum(out_in[...].astype(F32), axis=0)

    terms.wait_send()
    shift.wait_send()
    for row in shares:
        for copy in row:
            copy.wait_send()
    for copy in stores:
        copy.wait()

    def drain_far(i, carry):
        for copy in every[:4]:
            copy(i).wait_send()
        far_block(i).wait_send()
        return carry

    def drain_sum(i, carry):
        for copy in every[4:]:
            copy(i).wait_send()
        return carry

    def drain_near(i, carry):
        near_block(i, group).wait_send()
        return carry

    lax.fori_loop(1, far_last + 1, drain_far, 0)
    lax.fori_loop(0, chunks, drain_sum, 0)
    lax.fori_loop(far_last + 1, chunks, drain_near, 0)
    if group > 1:
        near_block(0, group - 1).wait_send()
    final.wait_send()


def run_step(dims, small, large):
    sps, tps, chunks, cap = dims
    cot, out_weight = small[2:4]
    gate = large[1]
    rows = sps * cap
    tokens = cot.shape[0]
    cols = cot.shape[1] // tps
    lane_w = out_weight.shape[1]
    width, units = gate.shape
    rows_c = rows // chunks
    vmem = pl.BlockSpec(memory_space=pltpu.VMEM)
    hbm = pl.BlockSpec(memory_space=pltpu.HBM)
    dma = pltpu.SemaphoreType.DMA
    scratch = [
        pltpu.VMEM((rows, cols), BF16),
        pltpu.VMEM((3 * rows_c, width), BF16),
        pltpu.VMEM((rows, tokens), BF16),
        pltpu.VMEM((rows, 1), F32),
        pltpu.VMEM((rows, cols), BF16),
        pltpu.VMEM((tokens, rows), BF16),
        pltpu.VMEM((tps, tokens, cols), BF16),
        pltpu.VMEM((tokens, lane_w), BF16),
        pltpu.VMEM((tokens + 8, lane_w), F32),
        pltpu.VMEM((tps, cols, lane_w), BF16),
        pltpu.VMEM((sps, width // sps, lane_w), BF16),
        pltpu.VMEM((width, units), BF16),
        pltpu.VMEM((width, units), BF16),
        pltpu.VMEM((units, width), BF16),
        pltpu.VMEM((rows, width), BF16),
        pltpu.VMEM((width, units), BF16),
        pltpu.VMEM((width, units), BF16),
        pltpu.VMEM((units, width), BF16),
        pltpu.VMEM((rows, width), BF16),
        pltpu.VMEM((tps, rows, cols), BF16),
        pltpu.VMEM((chunks, rows_c // 2, cols), BF16),
        pltpu.VMEM((chunks, rows_c // 2, cols), BF16),
        pltpu.VMEM((chunks, rows_c, cols), BF16),
        pltpu.VMEM((chunks, rows_c, cols), BF16),
        pltpu.VMEM((rows, cols), BF16),
        pltpu.VMEM((rows, units), F32),
        pltpu.VMEM((rows, units), F32),
        pltpu.VMEM((rows, units), BF16),
        pltpu.VMEM((rows, units), BF16),
        pltpu.VMEM((rows, units), BF16),
        dma((4,)),
        dma((3,)),
        dma((chunks,)),
        dma((chunks,)),
        dma((8, chunks)),
        dma((8, chunks)),
        dma,
        dma,
        dma((4, 2)),
        dma((4, 2)),
        dma,
        dma,
        dma,
        dma,
    ]
    outs = (
        ((tokens, cols), BF16),
        ((width, units), BF16),
        ((width, units), BF16),
        ((units, width), BF16),
        ((width // sps, lane_w), F32),
        ((tokens, lane_w), BF16),
        ((tokens, lane_w), BF16),
        ((tokens, lane_w), BF16),
    )
    return pl.pallas_call(
        functools.partial(step_kernel, dims),
        out_shape=tuple(jax.ShapeDtypeStruct(*out) for out in outs),
        in_specs=[vmem] * len(small) + [hbm] * len(large),
        out_specs=(vmem, hbm, hbm, hbm, vmem, vmem, vmem, vmem),
        scratch_shapes=scratch,
        compiler_params=pltpu.CompilerParams(
            collective_id=0, has_side_effects=True, vmem_limit_bytes=60 * 1024 * 1024
        ),
        name="step",
    )(*small, *large)


def store_kernel(count, *refs):
    given, results, held = refs[:count], refs[count : 2 * count], refs[2 * count : 3 * count]
    load_sem, store_sem = refs[3 * count :]
    loads = [pltpu.make_async_copy(given[n], held[n], load_sem.at[n]) for n in range(count)]
    stores = [pltpu.make_async_copy(held[n], results[n], store_sem.at[n]) for n in range(count)]
    for load in loads:
        load.start()
    for load, out in zip(loads, stores):
        load.wait()
        out.start()
    for out in stores:
        out.wait()


def store(values):
    count = len(values)
    hbm = pl.BlockSpec(memory_space=pltpu.HBM)
    dma = pltpu.SemaphoreType.DMA
    return pl.pallas_call(
        functools.partial(store_kernel, count),
        out_shape=tuple(jax.ShapeDtypeStruct(v.shape, v.dtype) for v in values),
        in_specs=[hbm] * count,
        out_specs=(hbm,) * count,
        scratch_shapes=[pltpu.VMEM(v.shape, v.dtype) for v in values]
        + [dma((count,)), dma((count,))],
        compiler_params=pltpu.CompilerParams(vmem_limit_bytes=60 * 1024 * 1024),
        name="store",
    )(*values)


def body(
    chunks,
    cotangent,
    route_ids,
    route_weights,
    expert_inputs,
    gate_weight,
    up_weight,
    down_weight,
    out_weight,
    gate_in,
    conv_sum,
    conv_c,
    conv_v,
    conv_taps,
):
    groups = lax.axis_size("sp")
    lanes = lax.axis_size("tp")
    capacity = expert_inputs.shape[1] // groups
    results = run_step(
        (groups, lanes, chunks, capacity),
        (
            route_ids.T,
            route_weights.T,
            cotangent,
            out_weight,
            gate_in,
            conv_sum,
            conv_c,
            conv_v,
            conv_taps,
        ),
        (expert_inputs[0], gate_weight[0], up_weight[0], down_weight[0]),
    )
    grad_input, grad_gate, grad_up, grad_down, *rest = store(results)
    return (grad_input, grad_gate[None], grad_up[None], grad_down[None], *rest)


def solution(mesh):
    placed = (
        P("sp", None),
        P("sp", None),
        P("sp", None),
        P("sp", None, None),
        P("sp", None, "tp"),
        P("sp", None, "tp"),
        P("sp", "tp", None),
        P(None, "tp"),
        P("sp", "tp"),
        P("sp", "tp"),
        P("sp", "tp"),
        P("sp", "tp"),
        P(None, "tp"),
    )
    chunks = 8
    return jax.shard_map(
        functools.partial(body, chunks),
        mesh=mesh,
        in_specs=placed,
        out_specs=(
            P("sp", "tp"),
            P("sp", None, "tp"),
            P("sp", None, "tp"),
            P("sp", "tp", None),
            P("sp", "tp"),
            P("sp", "tp"),
            P("sp", "tp"),
            P("sp", "tp"),
        ),
        check_vma=False,
    )
```

```python
import functools

import jax
import jax.numpy as jnp
from jax import lax
from jax.experimental import pallas as pl
from jax.experimental.pallas import tpu as pltpu
from jax.sharding import PartitionSpec as P

MESH = pl.DeviceIdType.MESH
F32 = jnp.float32
BF16 = jnp.bfloat16


def step_kernel(
    dims,
    ids,
    weights,
    cot,
    out_weight,
    gate_in,
    conv_sum,
    conv_c,
    conv_v,
    taps,
    x_hbm,
    gate_hbm,
    up_hbm,
    down_hbm,
    grad_input,
    g_gate_hbm,
    g_up_hbm,
    g_down_hbm,
    g_out,
    g_gate_in,
    g_conv_c,
    g_conv_v,
    out_ref,
    near_ref,
    chosen,
    slot_weight,
    returned,
    chosen_t,
    full_in,
    mixed,
    sums,
    out_terms,
    out_in,
    g_gate,
    g_up,
    g_down,
    x_v,
    gate_v,
    up_v,
    down_v,
    routed,
    part,
    rs1a,
    rs1b,
    rs2a,
    rs2b,
    ret_src,
    swish_s,
    slope_s,
    hidden_s,
    gpg_s,
    gpu_s,
    load_sem,
    store_sem,
    send_z,
    recv_z,
    send_y,
    recv_y,
    send_r,
    recv_r,
    send_s,
    recv_s,
    send_o,
    recv_o,
    send_n,
    recv_n,
):
    sps, tps, chunks, cap = dims
    near = 2
    group = sps // chunks
    rows_c = group * cap
    half = rows_c // 2
    cols = out_ref.shape[1]
    tokens = cot.shape[0]
    rows_all = sps * cap
    me = lax.axis_index("sp")
    q = lax.axis_index("tp")
    z = me // group
    g = me % group
    up_q = (q + 1) % tps
    dn_q = (q + tps - 1) % tps
    far_q = (q + 2) % tps

    loads = [
        pltpu.make_async_copy(src, dst, load_sem.at[n])
        for n, (src, dst) in enumerate(
            ((x_hbm, x_v), (gate_hbm, gate_v), (up_hbm, up_v), (down_hbm, down_v))
        )
    ]
    for load in loads:
        load.start()

    barrier = pltpu.get_barrier_semaphore()

    def greet(k, carry):
        pl.semaphore_signal(
            barrier, inc=1, device_id=((me + k) % sps, q), device_id_type=MESH
        )
        return carry

    lax.fori_loop(1, sps, greet, 0)
    for peer in (up_q, dn_q):
        pl.semaphore_signal(barrier, inc=1, device_id=(me, peer), device_id_type=MESH)

    names = lax.broadcasted_iota(jnp.int32, (sps, tokens), 0)
    first, second = names == ids[0:1, :], names == ids[1:2, :]
    weight = jnp.where(first, weights[0:1, :], 0.0) + jnp.where(second, weights[1:2, :], 0.0)
    named = first | second
    earlier = lax.broadcasted_iota(jnp.int32, (tokens, tokens), 0) < lax.broadcasted_iota(
        jnp.int32, (tokens, tokens), 1
    )
    rank = jnp.dot(
        jnp.where(named, 1.0, 0.0).astype(BF16),
        jnp.where(earlier, 1.0, 0.0).astype(BF16),
        preferred_element_type=F32,
    ).astype(jnp.int32)
    rank = jnp.where(named, rank, -1)
    pick = rank[:, None, :] == lax.broadcasted_iota(jnp.int32, (sps, cap, tokens), 1)
    chosen[...] = jnp.where(pick, 1.0, 0.0).reshape(rows_all, tokens).astype(BF16)
    slot_weight[...] = jnp.sum(
        jnp.where(pick, weight[:, None, :], 0.0).reshape(rows_all, tokens), axis=1, keepdims=True
    )
    lane_span = pl.ds(pl.multiple_of(q * cols, cols), cols)

    def build_near(slot, step_z):
        rows = pl.ds(pl.multiple_of(((z + step_z) % chunks) * rows_c, rows_c), rows_c)
        near_ref[slot * rows_c : (slot + 1) * rows_c, :] = (
            slot_weight[rows, :]
            * jnp.dot(chosen[rows, :], cot[...], preferred_element_type=F32)
        ).astype(BF16)

    out_ref[...] = (
        slot_weight[...] * jnp.dot(chosen[...], cot[:, lane_span], preferred_element_type=F32)
    ).astype(BF16)
    pl.semaphore_wait(barrier, sps - 1 + 2)

    far_last = chunks - near - 1

    def offset(i):
        u = (i + chunks - 1) % chunks
        w = u // (chunks - 3)
        far = (2 + u // 2) * (1 - 2 * (u % 2))
        return ((i + chunks - 1) // chunks) * (
            (1 - w) * far + w * (1 - 2 * ((u - (chunks - 3)) % 2))
        )

    def chunk_start(i):
        return ((z - offset(i) + chunks) % chunks) * rows_c

    def peer_of(i, k):
        return ((z + offset(i) + chunks) % chunks) * group + (g + k) % group

    own = pl.ds(pl.multiple_of(me * cap, cap), cap)

    def near_copy(i, slot, k):
        row = slot * rows_c + ((g + k) % group) * cap
        return pltpu.make_async_remote_copy(
            src_ref=near_ref.at[pl.ds(pl.multiple_of(row, cap), cap), :],
            dst_ref=routed.at[own, :],
            send_sem=send_z.at[i],
            recv_sem=recv_z.at[i],
            device_id=(peer_of(i, k), q),
            device_id_type=MESH,
        )

    def far_copy(i, k):
        peer = peer_of(i, k)
        return pltpu.make_async_remote_copy(
            src_ref=out_ref.at[pl.ds(pl.multiple_of(peer * cap, cap), cap), :],
            dst_ref=routed.at[own, lane_span],
            send_sem=send_z.at[i],
            recv_sem=recv_z.at[i],
            device_id=(peer, q),
            device_id_type=MESH,
        )

    def send_own(k, carry):
        far_copy(0, k).start()
        return carry

    def send_far(i, carry):
        def send_one(k, inner):
            far_copy(i, k).start()
            return inner

        return lax.fori_loop(0, group, send_one, carry)

    def send_near(i, carry):
        def send_one(k, inner):
            near_copy(i, i - far_last - 1, k).start()
            return inner

        return lax.fori_loop(0, group, send_one, carry)

    lax.fori_loop(1, group, send_own, 0)
    lax.fori_loop(1, 4, send_far, 0)
    routed[own, lane_span] = out_ref[own, :]
    build_near(0, 1)
    build_near(1, chunks - 1)

    chosen_t[...] = chosen[...].T
    mixed[...] = (gate_in[...].astype(F32) * conv_sum[...].astype(F32)).astype(BF16)

    for load in loads:
        load.wait()

    def at(i, first=0, size=None):
        return pl.ds(pl.multiple_of(chunk_start(i) + first, half), size or rows_c)

    def forward(i):
        rows = at(i)
        pre_gate = jnp.dot(x_v[rows, :], gate_v[...], preferred_element_type=F32)
        pre_up = jnp.dot(x_v[rows, :], up_v[...], preferred_element_type=F32)
        sig = jax.nn.sigmoid(pre_gate)
        swish = pre_gate * sig
        swish_s[rows, :] = swish
        slope_s[rows, :] = pre_up * sig * (1.0 + pre_gate * (1.0 - sig))
        hidden_s[rows, :] = (swish * pre_up).astype(BF16)

    def y_copy(src, dst, kind, i, peer):
        return pltpu.make_async_remote_copy(
            src_ref=src,
            dst_ref=dst,
            send_sem=send_y.at[kind, i],
            recv_sem=recv_y.at[kind, i],
            device_id=(me, peer),
            device_id_type=MESH,
        )

    def lanes_of(lane):
        return pl.ds(pl.multiple_of(lane * cols, cols), cols)

    def gather_up(i):
        ref = routed.at[at(i), lanes_of(q)]
        return y_copy(ref, ref, 0, i, up_q)

    def gather_dn(i):
        ref = routed.at[at(i), lanes_of(q)]
        return y_copy(ref, ref, 1, i, dn_q)

    def pass_up(i):
        ref = routed.at[at(i, 0, half), lanes_of(dn_q)]
        return y_copy(ref, ref, 2, i, up_q)

    def pass_dn(i):
        ref = routed.at[at(i, half, half), lanes_of(up_q)]
        return y_copy(ref, ref, 3, i, dn_q)

    def first_up(i):
        return y_copy(part.at[far_q, at(i, 0, half), :], rs1a.at[i], 4, i, up_q)

    def first_dn(i):
        return y_copy(part.at[far_q, at(i, half, half), :], rs1b.at[i], 5, i, dn_q)

    def last_up(i):
        return y_copy(part.at[up_q, at(i), :], rs2a.at[i], 6, i, up_q)

    def last_dn(i):
        return y_copy(part.at[dn_q, at(i), :], rs2b.at[i], 7, i, dn_q)

    every = (gather_up, gather_dn, pass_up, pass_dn, first_up, first_dn, last_up, last_dn)

    def far_block(i, count):
        rows = pl.ds(0, count * cap)
        return pltpu.make_async_remote_copy(
            src_ref=out_ref.at[rows, :],
            dst_ref=routed.at[rows, lane_span],
            send_sem=send_z.at[i],
            recv_sem=recv_z.at[i],
            device_id=(me, up_q),
            device_id_type=MESH,
        )

    def near_block(i):
        rows = pl.ds(0, rows_c)
        return pltpu.make_async_remote_copy(
            src_ref=near_ref.at[rows, :],
            dst_ref=routed.at[rows, :],
            send_sem=send_z.at[i],
            recv_sem=recv_z.at[i],
            device_id=(me, up_q),
            device_id_type=MESH,
        )

    def stage_gather(i):
        if group > 1:

            @pl.when(i == 0)
            def _():
                far_block(0, group - 1).wait_recv()

        @pl.when(i > 0)
        def _():
            far_block(i, group).wait_recv()

        gather_up(i).start()
        gather_dn(i).start()

        @pl.when((i > 0) & (i + 3 <= far_last))
        def _():
            send_far(i + 3, 0)

        @pl.when((i + 3 > far_last) & (i + 3 < chunks))
        def _():
            send_near(i + 3, 0)

    def stage_pass(i):
        gather_up(i).wait_recv()
        pass_up(i).start()
        gather_dn(i).wait_recv()
        pass_dn(i).start()

    def compute(i):
        rows = at(i)
        grad_hidden = jnp.zeros((rows_c, down_v.shape[0]), F32)
        for lane in range(tps):
            grad_hidden += lax.dot_general(
                routed[rows, lane * cols : (lane + 1) * cols],
                down_v[:, lane * cols : (lane + 1) * cols],
                (((1,), (1,)), ((), ())),
                preferred_element_type=F32,
            )
        gpg = (grad_hidden * slope_s[rows, :]).astype(BF16)
        gpu = (grad_hidden * swish_s[rows, :]).astype(BF16)
        gpg_s[rows, :] = gpg
        gpu_s[rows, :] = gpu
        for lane in range(tps):
            span = slice(lane * cols, (lane + 1) * cols)
            piece = lax.dot_general(
                gpg, gate_v[span, :], (((1,), (1,)), ((), ())), preferred_element_type=F32
            )
            piece += lax.dot_general(
                gpu, up_v[span, :], (((1,), (1,)), ((), ())), preferred_element_type=F32
            )
            part[lane, rows, :] = piece.astype(BF16)
        first_up(i).start()
        first_dn(i).start()

    def stage_compute(i):
        @pl.when(i <= far_last)
        def _():
            pass_up(i).wait_recv()
            pass_dn(i).wait_recv()

        @pl.when(i > far_last)
        def _():
            near_block(i).wait_recv()

        compute(i)

    def stage_first(i):
        lower, upper = at(i, 0, half), at(i, half, half)
        first_up(i).wait_recv()
        part[up_q, lower, :] = (
            part[up_q, lower, :].astype(F32) + rs1a[i].astype(F32)
        ).astype(BF16)
        last_up(i).start()
        first_dn(i).wait_recv()
        part[dn_q, upper, :] = (
            part[dn_q, upper, :].astype(F32) + rs1b[i].astype(F32)
        ).astype(BF16)
        last_dn(i).start()

    def return_copy(i, k):
        source = ((z - offset(i) + chunks) % chunks) * group + (g + k) % group
        return pltpu.make_async_remote_copy(
            src_ref=ret_src.at[pl.ds(pl.multiple_of(source * cap, cap), cap), :],
            dst_ref=returned.at[own, :],
            send_sem=send_r,
            recv_sem=recv_r,
            device_id=(source, q),
            device_id_type=MESH,
        )

    def stage_return(i):
        rows = at(i)
        last_up(i).wait_recv()
        last_dn(i).wait_recv()
        total = part[q, rows, :].astype(F32) + rs2a[i].astype(F32) + rs2b[i].astype(F32)
        ret_src[rows, :] = total.astype(BF16)

        @pl.when(i > 0)
        def _():
            return_copy(i, 0).start()

        def send_one(k, carry):
            return_copy(i, k).start()
            return carry

        lax.fori_loop(1, group, send_one, 0)

    forward(0)

    def step(t, carry):
        for stage, lead, first, last in (
            (stage_gather, 0, 0, far_last),
            (stage_pass, -1, 0, far_last),
            (stage_compute, -2, 0, chunks - 1),
            (forward, 1, 1, chunks - 1),
            (stage_first, -3, 0, chunks - 1),
            (stage_return, -4, 0, chunks - 1),
        ):
            i = t + lead

            @pl.when((i >= first) & (i <= last))
            def _():
                stage(i)

        return carry

    lax.fori_loop(0, chunks + 4, step, 0)
    returned[own, :] = ret_src[own, :]
    rest = pl.ds(0, (sps - 1) * cap)
    final = pltpu.make_async_remote_copy(
        src_ref=ret_src.at[rest, :],
        dst_ref=returned.at[rest, :],
        send_sem=send_r,
        recv_sem=recv_r,
        device_id=(me, up_q),
        device_id_type=MESH,
    )
    contract0 = (((0,), (0,)), ((), ()))
    stores = [
        pltpu.make_async_copy(src, dst, store_sem.at[n])
        for n, (src, dst) in enumerate(
            ((g_down, g_down_hbm), (g_gate, g_gate_hbm), (g_up, g_up_hbm))
        )
    ]
    for lane in range(tps):
        span = slice(lane * cols, (lane + 1) * cols)
        g_down[:, span] = lax.dot_general(
            hidden_s[...], routed[:, span], contract0, preferred_element_type=F32
        ).astype(BF16)
    stores[0].start()
    for lane in range(tps):
        span = slice(lane * cols, (lane + 1) * cols)
        g_gate[span, :] = lax.dot_general(
            x_v[:, span], gpg_s[...], contract0, preferred_element_type=F32
        ).astype(BF16)
    stores[1].start()
    final.wait_recv()

    pieces = 4
    wide = cols // pieces
    split = tokens // 2

    def share(lane, piece, first, size, kind, peer):
        ref = full_in.at[lane, pl.ds(first, size), pl.ds(piece * wide, wide)]
        return pltpu.make_async_remote_copy(
            src_ref=ref,
            dst_ref=ref,
            send_sem=send_s.at[kind, piece],
            recv_sem=recv_s.at[kind, piece],
            device_id=(me, peer),
            device_id_type=MESH,
        )

    shares = [
        (
            share(q, piece, 0, tokens, 0, up_q),
            share(q, piece, 0, tokens, 1, dn_q),
            share(dn_q, piece, 0, split, 2, up_q),
            share(up_q, piece, split, split, 3, dn_q),
        )
        for piece in range(pieces)
    ]
    per_lane = sps // tps
    per_piece = per_lane // pieces
    owned = g_out.shape[0]

    def send_terms(lane, piece):
        span = slice(piece * wide, (piece + 1) * wide)
        out_terms[lane, span, :] = lax.dot_general(
            full_in[lane, :, span], mixed[...], contract0, preferred_element_type=F32
        ).astype(BF16)

        def send_one(k, carry):
            place = piece * per_piece + (g + k) % per_piece
            owner = lane * per_lane + place
            block = pl.ds(pl.multiple_of(place * owned, owned), owned)

            @pl.when(owner != me)
            def _():
                pltpu.make_async_remote_copy(
                    src_ref=out_terms.at[lane, block, :],
                    dst_ref=out_in.at[me],
                    send_sem=send_o,
                    recv_sem=recv_o,
                    device_id=(owner, q),
                    device_id_type=MESH,
                ).start()

            @pl.when(owner == me)
            def _():
                out_in[me] = out_terms[lane, block, :]

            return carry

        lax.fori_loop(0, per_piece, send_one, 0)

    for piece in range(pieces):
        span = slice(piece * wide, (piece + 1) * wide)
        own_cols = pl.ds(pl.multiple_of(q * cols + piece * wide, wide), wide)
        own_grad = (
            cot[:, own_cols].astype(F32)
            + jnp.dot(chosen_t[...], returned[:, span], preferred_element_type=F32)
        ).astype(BF16)
        grad_input[:, span] = own_grad
        full_in[q, :, span] = own_grad
        shares[piece][0].start()
        shares[piece][1].start()
    for piece in range(pieces):
        send_terms(q, piece)
    for lane in range(tps):
        span = slice(lane * cols, (lane + 1) * cols)
        g_up[span, :] = lax.dot_general(
            x_v[:, span], gpu_s[...], contract0, preferred_element_type=F32
        ).astype(BF16)
    stores[2].start()

    for piece in range(pieces):
        shares[piece][0].wait_recv()
        shares[piece][2].start()
        shares[piece][1].wait_recv()
        shares[piece][3].start()
        send_terms(dn_q, piece)
        send_terms(up_q, piece)
    for piece in range(pieces):
        shares[piece][2].wait_recv()
        shares[piece][3].wait_recv()
        send_terms(far_q, piece)

    grad_mixed = jnp.zeros((tokens, out_weight.shape[1]), F32)
    for lane in range(tps):
        grad_mixed += jnp.dot(
            full_in[lane],
            out_weight[lane * cols : (lane + 1) * cols, :],
            preferred_element_type=F32,
        )
    sums[0:tokens, :] = grad_mixed * gate_in[...].astype(F32)
    edge = sums.shape[0] - tokens
    shift = pltpu.make_async_remote_copy(
        src_ref=sums.at[pl.ds(0, edge), :],
        dst_ref=sums.at[pl.ds(tokens, edge), :],
        send_sem=send_n,
        recv_sem=recv_n,
        device_id=((me + sps - 1) % sps, q),
        device_id_type=MESH,
    )
    shift.start()
    g_gate_in[...] = (grad_mixed * conv_sum[...].astype(F32)).astype(BF16)
    shift.wait_recv()

    @pl.when(me == sps - 1)
    def _():
        sums[tokens : tokens + edge, :] = jnp.zeros((edge, sums.shape[1]), F32)

    grad_prod = (
        taps[0:1, :] * sums[2 : tokens + 2, :]
        + taps[1:2, :] * sums[1 : tokens + 1, :]
        + taps[2:3, :] * sums[0:tokens, :]
    )
    g_conv_c[...] = (grad_prod * conv_v[...].astype(F32)).astype(BF16)
    g_conv_v[...] = (grad_prod * conv_c[...].astype(F32)).astype(BF16)

    others = out_in.at[pl.ds(0, sps - 1)]
    terms = pltpu.make_async_remote_copy(
        src_ref=others,
        dst_ref=others,
        send_sem=send_o,
        recv_sem=recv_o,
        device_id=(me, up_q),
        device_id_type=MESH,
    )
    terms.wait_recv()
    g_out[...] = jnp.sum(out_in[...].astype(F32), axis=0)

    terms.wait_send()
    shift.wait_send()
    for row in shares:
        for copy in row:
            copy.wait_send()
    for copy in stores:
        copy.wait()

    def drain_far(i, carry):
        for copy in every[:4]:
            copy(i).wait_send()

        @pl.when(i > 0)
        def _():
            far_block(i, group).wait_send()

        return carry

    def drain_sum(i, carry):
        for copy in every[4:]:
            copy(i).wait_send()
        return carry

    def drain_near(i, carry):
        near_block(i).wait_send()
        return carry

    lax.fori_loop(0, far_last + 1, drain_far, 0)
    lax.fori_loop(0, chunks, drain_sum, 0)
    lax.fori_loop(far_last + 1, chunks, drain_near, 0)
    if group > 1:
        far_block(0, group - 1).wait_send()
    final.wait_send()


def run_step(dims, small, large):
    sps, tps, chunks, cap = dims
    cot, out_weight = small[2:4]
    gate = large[1]
    rows = sps * cap
    tokens = cot.shape[0]
    cols = cot.shape[1] // tps
    lane_w = out_weight.shape[1]
    width, units = gate.shape
    rows_c = rows // chunks
    vmem = pl.BlockSpec(memory_space=pltpu.VMEM)
    hbm = pl.BlockSpec(memory_space=pltpu.HBM)
    dma = pltpu.SemaphoreType.DMA
    scratch = [
        pltpu.VMEM((rows, cols), BF16),
        pltpu.VMEM((2 * rows_c, width), BF16),
        pltpu.VMEM((rows, tokens), BF16),
        pltpu.VMEM((rows, 1), F32),
        pltpu.VMEM((rows, cols), BF16),
        pltpu.VMEM((tokens, rows), BF16),
        pltpu.VMEM((tps, tokens, cols), BF16),
        pltpu.VMEM((tokens, lane_w), BF16),
        pltpu.VMEM((tokens + 8, lane_w), F32),
        pltpu.VMEM((tps, cols, lane_w), BF16),
        pltpu.VMEM((sps, width // sps, lane_w), BF16),
        pltpu.VMEM((width, units), BF16),
        pltpu.VMEM((width, units), BF16),
        pltpu.VMEM((units, width), BF16),
        pltpu.VMEM((rows, width), BF16),
        pltpu.VMEM((width, units), BF16),
        pltpu.VMEM((width, units), BF16),
        pltpu.VMEM((units, width), BF16),
        pltpu.VMEM((rows, width), BF16),
        pltpu.VMEM((tps, rows, cols), BF16),
        pltpu.VMEM((chunks, rows_c // 2, cols), BF16),
        pltpu.VMEM((chunks, rows_c // 2, cols), BF16),
        pltpu.VMEM((chunks, rows_c, cols), BF16),
        pltpu.VMEM((chunks, rows_c, cols), BF16),
        pltpu.VMEM((rows, cols), BF16),
        pltpu.VMEM((rows, units), F32),
        pltpu.VMEM((rows, units), F32),
        pltpu.VMEM((rows, units), BF16),
        pltpu.VMEM((rows, units), BF16),
        pltpu.VMEM((rows, units), BF16),
        dma((4,)),
        dma((3,)),
        dma((chunks,)),
        dma((chunks,)),
        dma((8, chunks)),
        dma((8, chunks)),
        dma,
        dma,
        dma((4, 4)),
        dma((4, 4)),
        dma,
        dma,
        dma,
        dma,
    ]
    outs = (
        ((tokens, cols), BF16),
        ((width, units), BF16),
        ((width, units), BF16),
        ((units, width), BF16),
        ((width // sps, lane_w), F32),
        ((tokens, lane_w), BF16),
        ((tokens, lane_w), BF16),
        ((tokens, lane_w), BF16),
    )
    return pl.pallas_call(
        functools.partial(step_kernel, dims),
        out_shape=tuple(jax.ShapeDtypeStruct(*out) for out in outs),
        in_specs=[vmem] * len(small) + [hbm] * len(large),
        out_specs=(vmem, hbm, hbm, hbm, vmem, vmem, vmem, vmem),
        scratch_shapes=scratch,
        compiler_params=pltpu.CompilerParams(
            collective_id=0, has_side_effects=True, vmem_limit_bytes=60 * 1024 * 1024
        ),
        name="step",
    )(*small, *large)


def store_kernel(count, *refs):
    given, results, held = refs[:count], refs[count : 2 * count], refs[2 * count : 3 * count]
    load_sem, store_sem = refs[3 * count :]
    loads = [pltpu.make_async_copy(given[n], held[n], load_sem.at[n]) for n in range(count)]
    stores = [pltpu.make_async_copy(held[n], results[n], store_sem.at[n]) for n in range(count)]
    for load in loads:
        load.start()
    for load, out in zip(loads, stores):
        load.wait()
        out.start()
    for out in stores:
        out.wait()


def store(values):
    count = len(values)
    hbm = pl.BlockSpec(memory_space=pltpu.HBM)
    dma = pltpu.SemaphoreType.DMA
    return pl.pallas_call(
        functools.partial(store_kernel, count),
        out_shape=tuple(jax.ShapeDtypeStruct(v.shape, v.dtype) for v in values),
        in_specs=[hbm] * count,
        out_specs=(hbm,) * count,
        scratch_shapes=[pltpu.VMEM(v.shape, v.dtype) for v in values]
        + [dma((count,)), dma((count,))],
        compiler_params=pltpu.CompilerParams(vmem_limit_bytes=60 * 1024 * 1024),
        name="store",
    )(*values)


def body(
    chunks,
    cotangent,
    route_ids,
    route_weights,
    expert_inputs,
    gate_weight,
    up_weight,
    down_weight,
    out_weight,
    gate_in,
    conv_sum,
    conv_c,
    conv_v,
    conv_taps,
):
    groups = lax.axis_size("sp")
    lanes = lax.axis_size("tp")
    capacity = expert_inputs.shape[1] // groups
    results = run_step(
        (groups, lanes, chunks, capacity),
        (
            route_ids.T,
            route_weights.T,
            cotangent,
            out_weight,
            gate_in,
            conv_sum,
            conv_c,
            conv_v,
            conv_taps,
        ),
        (expert_inputs[0], gate_weight[0], up_weight[0], down_weight[0]),
    )
    grad_input, grad_gate, grad_up, grad_down, *rest = store(results)
    return (grad_input, grad_gate[None], grad_up[None], grad_down[None], *rest)


def solution(mesh):
    placed = (
        P("sp", None),
        P("sp", None),
        P("sp", None),
        P("sp", None, None),
        P("sp", None, "tp"),
        P("sp", None, "tp"),
        P("sp", "tp", None),
        P(None, "tp"),
        P("sp", "tp"),
        P("sp", "tp"),
        P("sp", "tp"),
        P("sp", "tp"),
        P(None, "tp"),
    )
    chunks = 8
    return jax.shard_map(
        functools.partial(body, chunks),
        mesh=mesh,
        in_specs=placed,
        out_specs=(
            P("sp", "tp"),
            P("sp", None, "tp"),
            P("sp", None, "tp"),
            P("sp", "tp", None),
            P("sp", "tp"),
            P("sp", "tp"),
            P("sp", "tp"),
            P("sp", "tp"),
        ),
        check_vma=False,
    )
```

```python
import functools

import jax
import jax.numpy as jnp
from jax import lax
from jax.experimental import pallas as pl
from jax.experimental.pallas import tpu as pltpu
from jax.sharding import PartitionSpec as P

MESH = pl.DeviceIdType.MESH
F32 = jnp.float32
BF16 = jnp.bfloat16


def step_kernel(
    dims,
    ids,
    weights,
    cot,
    taps,
    out_weight_hbm,
    gate_in_hbm,
    conv_sum_hbm,
    conv_c_hbm,
    conv_v_hbm,
    x_hbm,
    gate_hbm,
    up_hbm,
    down_hbm,
    grad_input_hbm,
    g_gate_hbm,
    g_up_hbm,
    g_down_hbm,
    g_out_hbm,
    g_gate_in_hbm,
    g_conv_c_hbm,
    g_conv_v_hbm,
    out_weight,
    gate_in,
    conv_sum,
    conv_c,
    conv_v,
    grad_input,
    g_out,
    g_gate_in,
    g_conv_c,
    g_conv_v,
    out_ref,
    near_ref,
    chosen,
    slot_weight,
    returned,
    chosen_t,
    full_in,
    mixed,
    sums,
    out_terms,
    out_in,
    g_gate,
    g_up,
    g_down,
    x_v,
    gate_v,
    up_v,
    down_v,
    routed,
    part,
    rs1a,
    rs1b,
    rs2a,
    rs2b,
    ret_src,
    swish_s,
    slope_s,
    hidden_s,
    gpg_s,
    gpu_s,
    load_sem,
    store_sem,
    send_z,
    recv_z,
    send_y,
    recv_y,
    send_r,
    recv_r,
    send_s,
    recv_s,
    send_o,
    recv_o,
    send_n,
    recv_n,
):
    sps, tps, chunks, cap = dims
    near = 2
    group = sps // chunks
    rows_c = group * cap
    half = rows_c // 2
    cols = out_ref.shape[1]
    tokens = cot.shape[0]
    rows_all = sps * cap
    me = lax.axis_index("sp")
    q = lax.axis_index("tp")
    z = me // group
    g = me % group
    up_q = (q + 1) % tps
    dn_q = (q + tps - 1) % tps
    far_q = (q + 2) % tps

    loads = [
        pltpu.make_async_copy(src, dst, load_sem.at[n])
        for n, (src, dst) in enumerate(
            (
                (x_hbm, x_v),
                (gate_hbm, gate_v),
                (up_hbm, up_v),
                (down_hbm, down_v),
                (gate_in_hbm, gate_in),
                (conv_sum_hbm, conv_sum),
                (conv_c_hbm, conv_c),
                (conv_v_hbm, conv_v),
                (out_weight_hbm, out_weight),
            )
        )
    ]
    for load in loads:
        load.start()

    barrier = pltpu.get_barrier_semaphore()

    def greet(k, carry):
        pl.semaphore_signal(
            barrier, inc=1, device_id=((me + k) % sps, q), device_id_type=MESH
        )
        return carry

    lax.fori_loop(1, sps, greet, 0)
    for peer in (up_q, dn_q):
        pl.semaphore_signal(barrier, inc=1, device_id=(me, peer), device_id_type=MESH)

    names = lax.broadcasted_iota(jnp.int32, (sps, tokens), 0)
    first, second = names == ids[0:1, :], names == ids[1:2, :]
    weight = jnp.where(first, weights[0:1, :], 0.0) + jnp.where(second, weights[1:2, :], 0.0)
    named = first | second
    earlier = lax.broadcasted_iota(jnp.int32, (tokens, tokens), 0) < lax.broadcasted_iota(
        jnp.int32, (tokens, tokens), 1
    )
    rank = jnp.dot(
        jnp.where(named, 1.0, 0.0).astype(BF16),
        jnp.where(earlier, 1.0, 0.0).astype(BF16),
        preferred_element_type=F32,
    ).astype(jnp.int32)
    rank = jnp.where(named, rank, -1)
    pick = rank[:, None, :] == lax.broadcasted_iota(jnp.int32, (sps, cap, tokens), 1)
    chosen[...] = jnp.where(pick, 1.0, 0.0).reshape(rows_all, tokens).astype(BF16)
    slot_weight[...] = jnp.sum(
        jnp.where(pick, weight[:, None, :], 0.0).reshape(rows_all, tokens), axis=1, keepdims=True
    )
    lane_span = pl.ds(pl.multiple_of(q * cols, cols), cols)

    def build_near(slot, step_z):
        rows = pl.ds(pl.multiple_of(((z + step_z) % chunks) * rows_c, rows_c), rows_c)
        near_ref[slot * rows_c : (slot + 1) * rows_c, :] = (
            slot_weight[rows, :]
            * jnp.dot(chosen[rows, :], cot[...], preferred_element_type=F32)
        ).astype(BF16)

    out_ref[...] = (
        slot_weight[...] * jnp.dot(chosen[...], cot[:, lane_span], preferred_element_type=F32)
    ).astype(BF16)
    pl.semaphore_wait(barrier, sps - 1 + 2)

    far_last = chunks - near - 1

    def offset(i):
        u = (i + chunks - 1) % chunks
        w = u // (chunks - 3)
        far = (2 + u // 2) * (1 - 2 * (u % 2))
        return ((i + chunks - 1) // chunks) * (
            (1 - w) * far + w * (1 - 2 * ((u - (chunks - 3)) % 2))
        )

    def chunk_start(i):
        return ((z - offset(i) + chunks) % chunks) * rows_c

    def peer_of(i, k):
        return ((z + offset(i) + chunks) % chunks) * group + (g + k) % group

    own = pl.ds(pl.multiple_of(me * cap, cap), cap)

    def near_copy(i, slot, k):
        row = slot * rows_c + ((g + k) % group) * cap
        return pltpu.make_async_remote_copy(
            src_ref=near_ref.at[pl.ds(pl.multiple_of(row, cap), cap), :],
            dst_ref=routed.at[own, :],
            send_sem=send_z.at[i],
            recv_sem=recv_z.at[i],
            device_id=(peer_of(i, k), q),
            device_id_type=MESH,
        )

    def far_copy(i, k):
        peer = peer_of(i, k)
        return pltpu.make_async_remote_copy(
            src_ref=out_ref.at[pl.ds(pl.multiple_of(peer * cap, cap), cap), :],
            dst_ref=routed.at[own, lane_span],
            send_sem=send_z.at[i],
            recv_sem=recv_z.at[i],
            device_id=(peer, q),
            device_id_type=MESH,
        )

    def send_own(k, carry):
        far_copy(0, k).start()
        return carry

    def send_far(i, carry):
        def send_one(k, inner):
            far_copy(i, k).start()
            return inner

        return lax.fori_loop(0, group, send_one, carry)

    def send_near(i, carry):
        def send_one(k, inner):
            near_copy(i, i - far_last - 1, k).start()
            return inner

        return lax.fori_loop(0, group, send_one, carry)

    lax.fori_loop(1, group, send_own, 0)
    lax.fori_loop(1, 4, send_far, 0)
    routed[own, lane_span] = out_ref[own, :]
    build_near(0, 1)
    build_near(1, chunks - 1)

    chosen_t[...] = chosen[...].T

    for load in loads:
        load.wait()
    mixed[...] = (gate_in[...].astype(F32) * conv_sum[...].astype(F32)).astype(BF16)

    def at(i, first=0, size=None):
        return pl.ds(pl.multiple_of(chunk_start(i) + first, half), size or rows_c)

    def forward(i):
        rows = at(i)
        pre_gate = jnp.dot(x_v[rows, :], gate_v[...], preferred_element_type=F32)
        pre_up = jnp.dot(x_v[rows, :], up_v[...], preferred_element_type=F32)
        sig = jax.nn.sigmoid(pre_gate)
        swish = pre_gate * sig
        swish_s[rows, :] = swish
        slope_s[rows, :] = pre_up * sig * (1.0 + pre_gate * (1.0 - sig))
        hidden_s[rows, :] = (swish * pre_up).astype(BF16)

    def y_copy(src, dst, kind, i, peer):
        return pltpu.make_async_remote_copy(
            src_ref=src,
            dst_ref=dst,
            send_sem=send_y.at[kind, i],
            recv_sem=recv_y.at[kind, i],
            device_id=(me, peer),
            device_id_type=MESH,
        )

    def lanes_of(lane):
        return pl.ds(pl.multiple_of(lane * cols, cols), cols)

    def gather_up(i):
        ref = routed.at[at(i), lanes_of(q)]
        return y_copy(ref, ref, 0, i, up_q)

    def gather_dn(i):
        ref = routed.at[at(i), lanes_of(q)]
        return y_copy(ref, ref, 1, i, dn_q)

    def pass_up(i):
        ref = routed.at[at(i, 0, half), lanes_of(dn_q)]
        return y_copy(ref, ref, 2, i, up_q)

    def pass_dn(i):
        ref = routed.at[at(i, half, half), lanes_of(up_q)]
        return y_copy(ref, ref, 3, i, dn_q)

    def first_up(i):
        return y_copy(part.at[far_q, at(i, 0, half), :], rs1a.at[i], 4, i, up_q)

    def first_dn(i):
        return y_copy(part.at[far_q, at(i, half, half), :], rs1b.at[i], 5, i, dn_q)

    def last_up(i):
        return y_copy(part.at[up_q, at(i), :], rs2a.at[i], 6, i, up_q)

    def last_dn(i):
        return y_copy(part.at[dn_q, at(i), :], rs2b.at[i], 7, i, dn_q)

    every = (gather_up, gather_dn, pass_up, pass_dn, first_up, first_dn, last_up, last_dn)

    def far_block(i, count):
        rows = pl.ds(0, count * cap)
        return pltpu.make_async_remote_copy(
            src_ref=out_ref.at[rows, :],
            dst_ref=routed.at[rows, lane_span],
            send_sem=send_z.at[i],
            recv_sem=recv_z.at[i],
            device_id=(me, up_q),
            device_id_type=MESH,
        )

    def near_block(i):
        rows = pl.ds(0, rows_c)
        return pltpu.make_async_remote_copy(
            src_ref=near_ref.at[rows, :],
            dst_ref=routed.at[rows, :],
            send_sem=send_z.at[i],
            recv_sem=recv_z.at[i],
            device_id=(me, up_q),
            device_id_type=MESH,
        )

    def stage_gather(i):
        if group > 1:

            @pl.when(i == 0)
            def _():
                far_block(0, group - 1).wait_recv()

        @pl.when(i > 0)
        def _():
            far_block(i, group).wait_recv()

        gather_up(i).start()
        gather_dn(i).start()

        @pl.when((i > 0) & (i + 3 <= far_last))
        def _():
            send_far(i + 3, 0)

        @pl.when((i + 3 > far_last) & (i + 3 < chunks))
        def _():
            send_near(i + 3, 0)

    def stage_pass(i):
        gather_up(i).wait_recv()
        pass_up(i).start()
        gather_dn(i).wait_recv()
        pass_dn(i).start()

    def compute(i):
        rows = at(i)
        grad_hidden = jnp.zeros((rows_c, down_v.shape[0]), F32)
        for lane in range(tps):
            grad_hidden += lax.dot_general(
                routed[rows, lane * cols : (lane + 1) * cols],
                down_v[:, lane * cols : (lane + 1) * cols],
                (((1,), (1,)), ((), ())),
                preferred_element_type=F32,
            )
        gpg = (grad_hidden * slope_s[rows, :]).astype(BF16)
        gpu = (grad_hidden * swish_s[rows, :]).astype(BF16)
        gpg_s[rows, :] = gpg
        gpu_s[rows, :] = gpu
        for lane in range(tps):
            span = slice(lane * cols, (lane + 1) * cols)
            piece = lax.dot_general(
                gpg, gate_v[span, :], (((1,), (1,)), ((), ())), preferred_element_type=F32
            )
            piece += lax.dot_general(
                gpu, up_v[span, :], (((1,), (1,)), ((), ())), preferred_element_type=F32
            )
            part[lane, rows, :] = piece.astype(BF16)
        first_up(i).start()
        first_dn(i).start()

    def stage_compute(i):
        @pl.when(i <= far_last)
        def _():
            pass_up(i).wait_recv()
            pass_dn(i).wait_recv()

        @pl.when(i > far_last)
        def _():
            near_block(i).wait_recv()

        compute(i)

    def stage_first(i):
        lower, upper = at(i, 0, half), at(i, half, half)
        first_up(i).wait_recv()
        part[up_q, lower, :] = (
            part[up_q, lower, :].astype(F32) + rs1a[i].astype(F32)
        ).astype(BF16)
        last_up(i).start()
        first_dn(i).wait_recv()
        part[dn_q, upper, :] = (
            part[dn_q, upper, :].astype(F32) + rs1b[i].astype(F32)
        ).astype(BF16)
        last_dn(i).start()

    def return_copy(i, k):
        source = ((z - offset(i) + chunks) % chunks) * group + (g + k) % group
        return pltpu.make_async_remote_copy(
            src_ref=ret_src.at[pl.ds(pl.multiple_of(source * cap, cap), cap), :],
            dst_ref=returned.at[own, :],
            send_sem=send_r,
            recv_sem=recv_r,
            device_id=(source, q),
            device_id_type=MESH,
        )

    def stage_return(i):
        rows = at(i)
        last_up(i).wait_recv()
        last_dn(i).wait_recv()
        total = part[q, rows, :].astype(F32) + rs2a[i].astype(F32) + rs2b[i].astype(F32)
        ret_src[rows, :] = total.astype(BF16)

        @pl.when(i > 0)
        def _():
            return_copy(i, 0).start()

        def send_one(k, carry):
            return_copy(i, k).start()
            return carry

        lax.fori_loop(1, group, send_one, 0)

    forward(0)

    def step(t, carry):
        for stage, lead, first, last in (
            (stage_gather, 0, 0, far_last),
            (stage_pass, -1, 0, far_last),
            (stage_compute, -2, 0, chunks - 1),
            (forward, 1, 1, chunks - 1),
            (stage_first, -3, 0, chunks - 1),
            (stage_return, -4, 0, chunks - 1),
        ):
            i = t + lead

            @pl.when((i >= first) & (i <= last))
            def _():
                stage(i)

        return carry

    lax.fori_loop(0, chunks + 4, step, 0)
    returned[own, :] = ret_src[own, :]
    rest = pl.ds(0, (sps - 1) * cap)
    final = pltpu.make_async_remote_copy(
        src_ref=ret_src.at[rest, :],
        dst_ref=returned.at[rest, :],
        send_sem=send_r,
        recv_sem=recv_r,
        device_id=(me, up_q),
        device_id_type=MESH,
    )
    contract0 = (((0,), (0,)), ((), ()))
    stores = [
        pltpu.make_async_copy(src, dst, store_sem.at[n])
        for n, (src, dst) in enumerate(
            (
                (g_down, g_down_hbm),
                (g_gate, g_gate_hbm),
                (g_up, g_up_hbm),
                (grad_input, grad_input_hbm),
                (g_gate_in, g_gate_in_hbm),
                (g_conv_c, g_conv_c_hbm),
                (g_conv_v, g_conv_v_hbm),
                (g_out, g_out_hbm),
            )
        )
    ]
    for lane in range(tps):
        span = slice(lane * cols, (lane + 1) * cols)
        g_down[:, span] = lax.dot_general(
            hidden_s[...], routed[:, span], contract0, preferred_element_type=F32
        ).astype(BF16)
    stores[0].start()
    for lane in range(tps):
        span = slice(lane * cols, (lane + 1) * cols)
        g_gate[span, :] = lax.dot_general(
            x_v[:, span], gpg_s[...], contract0, preferred_element_type=F32
        ).astype(BF16)
    stores[1].start()
    final.wait_recv()

    pieces = 4
    wide = cols // pieces
    split = tokens // 2

    def share(lane, piece, first, size, kind, peer):
        ref = full_in.at[lane, pl.ds(first, size), pl.ds(piece * wide, wide)]
        return pltpu.make_async_remote_copy(
            src_ref=ref,
            dst_ref=ref,
            send_sem=send_s.at[kind, piece],
            recv_sem=recv_s.at[kind, piece],
            device_id=(me, peer),
            device_id_type=MESH,
        )

    shares = [
        (
            share(q, piece, 0, tokens, 0, up_q),
            share(q, piece, 0, tokens, 1, dn_q),
            share(dn_q, piece, 0, split, 2, up_q),
            share(up_q, piece, split, split, 3, dn_q),
        )
        for piece in range(pieces)
    ]
    per_lane = sps // tps
    per_piece = per_lane // pieces
    owned = g_out.shape[0]

    def send_terms(lane, piece):
        span = slice(piece * wide, (piece + 1) * wide)
        out_terms[lane, span, :] = lax.dot_general(
            full_in[lane, :, span], mixed[...], contract0, preferred_element_type=F32
        ).astype(BF16)

        def send_one(k, carry):
            place = piece * per_piece + (g + k) % per_piece
            owner = lane * per_lane + place
            block = pl.ds(pl.multiple_of(place * owned, owned), owned)

            @pl.when(owner != me)
            def _():
                pltpu.make_async_remote_copy(
                    src_ref=out_terms.at[lane, block, :],
                    dst_ref=out_in.at[me],
                    send_sem=send_o,
                    recv_sem=recv_o,
                    device_id=(owner, q),
                    device_id_type=MESH,
                ).start()

            @pl.when(owner == me)
            def _():
                out_in[me] = out_terms[lane, block, :]

            return carry

        lax.fori_loop(0, per_piece, send_one, 0)

    for piece in range(pieces):
        span = slice(piece * wide, (piece + 1) * wide)
        own_cols = pl.ds(pl.multiple_of(q * cols + piece * wide, wide), wide)
        own_grad = (
            cot[:, own_cols].astype(F32)
            + jnp.dot(chosen_t[...], returned[:, span], preferred_element_type=F32)
        ).astype(BF16)
        grad_input[:, span] = own_grad
        full_in[q, :, span] = own_grad
        shares[piece][0].start()
        shares[piece][1].start()
    stores[3].start()
    for piece in range(pieces):
        send_terms(q, piece)
    for lane in range(tps):
        span = slice(lane * cols, (lane + 1) * cols)
        g_up[span, :] = lax.dot_general(
            x_v[:, span], gpu_s[...], contract0, preferred_element_type=F32
        ).astype(BF16)
    stores[2].start()

    for piece in range(pieces):
        shares[piece][0].wait_recv()
        shares[piece][2].start()
        shares[piece][1].wait_recv()
        shares[piece][3].start()
        send_terms(dn_q, piece)
        send_terms(up_q, piece)
    for piece in range(pieces):
        shares[piece][2].wait_recv()
        shares[piece][3].wait_recv()
        send_terms(far_q, piece)

    grad_mixed = jnp.zeros((tokens, out_weight.shape[1]), F32)
    for lane in range(tps):
        grad_mixed += jnp.dot(
            full_in[lane],
            out_weight[lane * cols : (lane + 1) * cols, :],
            preferred_element_type=F32,
        )
    sums[0:tokens, :] = grad_mixed * gate_in[...].astype(F32)
    edge = sums.shape[0] - tokens
    shift = pltpu.make_async_remote_copy(
        src_ref=sums.at[pl.ds(0, edge), :],
        dst_ref=sums.at[pl.ds(tokens, edge), :],
        send_sem=send_n,
        recv_sem=recv_n,
        device_id=((me + sps - 1) % sps, q),
        device_id_type=MESH,
    )
    shift.start()
    g_gate_in[...] = (grad_mixed * conv_sum[...].astype(F32)).astype(BF16)
    stores[4].start()
    shift.wait_recv()

    @pl.when(me == sps - 1)
    def _():
        sums[tokens : tokens + edge, :] = jnp.zeros((edge, sums.shape[1]), F32)

    grad_prod = (
        taps[0:1, :] * sums[2 : tokens + 2, :]
        + taps[1:2, :] * sums[1 : tokens + 1, :]
        + taps[2:3, :] * sums[0:tokens, :]
    )
    g_conv_c[...] = (grad_prod * conv_v[...].astype(F32)).astype(BF16)
    g_conv_v[...] = (grad_prod * conv_c[...].astype(F32)).astype(BF16)
    stores[5].start()
    stores[6].start()

    others = out_in.at[pl.ds(0, sps - 1)]
    terms = pltpu.make_async_remote_copy(
        src_ref=others,
        dst_ref=others,
        send_sem=send_o,
        recv_sem=recv_o,
        device_id=(me, up_q),
        device_id_type=MESH,
    )
    terms.wait_recv()
    g_out[...] = jnp.sum(out_in[...].astype(F32), axis=0)
    stores[7].start()

    terms.wait_send()
    shift.wait_send()
    for row in shares:
        for copy in row:
            copy.wait_send()
    for copy in stores:
        copy.wait()

    def drain_far(i, carry):
        for copy in every[:4]:
            copy(i).wait_send()

        @pl.when(i > 0)
        def _():
            far_block(i, group).wait_send()

        return carry

    def drain_sum(i, carry):
        for copy in every[4:]:
            copy(i).wait_send()
        return carry

    def drain_near(i, carry):
        near_block(i).wait_send()
        return carry

    lax.fori_loop(0, far_last + 1, drain_far, 0)
    lax.fori_loop(0, chunks, drain_sum, 0)
    lax.fori_loop(far_last + 1, chunks, drain_near, 0)
    if group > 1:
        far_block(0, group - 1).wait_send()
    final.wait_send()


def run_step(dims, small, large):
    sps, tps, chunks, cap = dims
    cot, out_weight = small[2], large[0]
    gate = large[6]
    rows = sps * cap
    tokens = cot.shape[0]
    cols = cot.shape[1] // tps
    lane_w = out_weight.shape[1]
    width, units = gate.shape
    rows_c = rows // chunks
    vmem = pl.BlockSpec(memory_space=pltpu.VMEM)
    hbm = pl.BlockSpec(memory_space=pltpu.HBM)
    dma = pltpu.SemaphoreType.DMA
    lane_bf16 = pltpu.VMEM((tokens, lane_w), BF16)
    scratch = [
        pltpu.VMEM((width, lane_w), BF16),
        lane_bf16,
        lane_bf16,
        lane_bf16,
        lane_bf16,
        pltpu.VMEM((tokens, cols), BF16),
        pltpu.VMEM((width // sps, lane_w), F32),
        lane_bf16,
        lane_bf16,
        lane_bf16,
        pltpu.VMEM((rows, cols), BF16),
        pltpu.VMEM((2 * rows_c, width), BF16),
        pltpu.VMEM((rows, tokens), BF16),
        pltpu.VMEM((rows, 1), F32),
        pltpu.VMEM((rows, cols), BF16),
        pltpu.VMEM((tokens, rows), BF16),
        pltpu.VMEM((tps, tokens, cols), BF16),
        pltpu.VMEM((tokens, lane_w), BF16),
        pltpu.VMEM((tokens + 8, lane_w), F32),
        pltpu.VMEM((tps, cols, lane_w), BF16),
        pltpu.VMEM((sps, width // sps, lane_w), BF16),
        pltpu.VMEM((width, units), BF16),
        pltpu.VMEM((width, units), BF16),
        pltpu.VMEM((units, width), BF16),
        pltpu.VMEM((rows, width), BF16),
        pltpu.VMEM((width, units), BF16),
        pltpu.VMEM((width, units), BF16),
        pltpu.VMEM((units, width), BF16),
        pltpu.VMEM((rows, width), BF16),
        pltpu.VMEM((tps, rows, cols), BF16),
        pltpu.VMEM((chunks, rows_c // 2, cols), BF16),
        pltpu.VMEM((chunks, rows_c // 2, cols), BF16),
        pltpu.VMEM((chunks, rows_c, cols), BF16),
        pltpu.VMEM((chunks, rows_c, cols), BF16),
        pltpu.VMEM((rows, cols), BF16),
        pltpu.VMEM((rows, units), F32),
        pltpu.VMEM((rows, units), F32),
        pltpu.VMEM((rows, units), BF16),
        pltpu.VMEM((rows, units), BF16),
        pltpu.VMEM((rows, units), BF16),
        dma((9,)),
        dma((8,)),
        dma((chunks,)),
        dma((chunks,)),
        dma((8, chunks)),
        dma((8, chunks)),
        dma,
        dma,
        dma((4, 4)),
        dma((4, 4)),
        dma,
        dma,
        dma,
        dma,
    ]
    outs = (
        ((tokens, cols), BF16),
        ((width, units), BF16),
        ((width, units), BF16),
        ((units, width), BF16),
        ((width // sps, lane_w), F32),
        ((tokens, lane_w), BF16),
        ((tokens, lane_w), BF16),
        ((tokens, lane_w), BF16),
    )
    return pl.pallas_call(
        functools.partial(step_kernel, dims),
        out_shape=tuple(jax.ShapeDtypeStruct(*out) for out in outs),
        in_specs=[vmem] * len(small) + [hbm] * len(large),
        out_specs=(hbm,) * len(outs),
        scratch_shapes=scratch,
        compiler_params=pltpu.CompilerParams(
            collective_id=0, has_side_effects=True, vmem_limit_bytes=60 * 1024 * 1024
        ),
        name="step",
    )(*small, *large)


def store_kernel(count, *refs):
    given, results, held = refs[:count], refs[count : 2 * count], refs[2 * count : 3 * count]
    load_sem, store_sem = refs[3 * count :]
    loads = [pltpu.make_async_copy(given[n], held[n], load_sem.at[n]) for n in range(count)]
    stores = [pltpu.make_async_copy(held[n], results[n], store_sem.at[n]) for n in range(count)]
    for load in loads:
        load.start()
    for load, out in zip(loads, stores):
        load.wait()
        out.start()
    for out in stores:
        out.wait()


def store(values):
    count = len(values)
    hbm = pl.BlockSpec(memory_space=pltpu.HBM)
    dma = pltpu.SemaphoreType.DMA
    return pl.pallas_call(
        functools.partial(store_kernel, count),
        out_shape=tuple(jax.ShapeDtypeStruct(v.shape, v.dtype) for v in values),
        in_specs=[hbm] * count,
        out_specs=(hbm,) * count,
        scratch_shapes=[pltpu.VMEM(v.shape, v.dtype) for v in values]
        + [dma((count,)), dma((count,))],
        compiler_params=pltpu.CompilerParams(vmem_limit_bytes=60 * 1024 * 1024),
        name="store",
    )(*values)


def body(
    chunks,
    cotangent,
    route_ids,
    route_weights,
    expert_inputs,
    gate_weight,
    up_weight,
    down_weight,
    out_weight,
    gate_in,
    conv_sum,
    conv_c,
    conv_v,
    conv_taps,
):
    groups = lax.axis_size("sp")
    lanes = lax.axis_size("tp")
    capacity = expert_inputs.shape[1] // groups
    results = run_step(
        (groups, lanes, chunks, capacity),
        (route_ids.T, route_weights.T, cotangent, conv_taps),
        (
            out_weight,
            gate_in,
            conv_sum,
            conv_c,
            conv_v,
            expert_inputs[0],
            gate_weight[0],
            up_weight[0],
            down_weight[0],
        ),
    )
    grad_input, grad_gate, grad_up, grad_down, *rest = store(results)
    return (grad_input, grad_gate[None], grad_up[None], grad_down[None], *rest)


def solution(mesh):
    placed = (
        P("sp", None),
        P("sp", None),
        P("sp", None),
        P("sp", None, None),
        P("sp", None, "tp"),
        P("sp", None, "tp"),
        P("sp", "tp", None),
        P(None, "tp"),
        P("sp", "tp"),
        P("sp", "tp"),
        P("sp", "tp"),
        P("sp", "tp"),
        P(None, "tp"),
    )
    chunks = 8
    return jax.shard_map(
        functools.partial(body, chunks),
        mesh=mesh,
        in_specs=placed,
        out_specs=(
            P("sp", "tp"),
            P("sp", None, "tp"),
            P("sp", None, "tp"),
            P("sp", "tp", None),
            P("sp", "tp"),
            P("sp", "tp"),
            P("sp", "tp"),
            P("sp", "tp"),
        ),
        check_vma=False,
    )
```
